256 devices in a mesh: ep: 32 (over z, x), tp: 8 (over y, core).
Axes of the slice: x: 4, y: 4, z: 8, core: 2. Of those that a mesh axis runs over, the one named last changes fastest.
Arguments:
- queries: bfloat16 [32768, 2048], P('ep', 'tp'), may hold values from -6 to 6
- key_vectors: bfloat16 [32768, 2048], P('ep', 'tp'), may hold values from -6 to 6
- value_vectors: bfloat16 [32768, 4096], P('ep', 'tp'), may hold values from -6 to 6
- decay_logit: float32 [32768, 2048], P('ep', 'tp'), may hold values from -11 to 16
- head_gain: float32 [256], replicated, may hold values from 0.1 to 1.9
- routed_rows: bfloat16 [8192, 4096], P('ep'), may hold values from -6 to 6
- pre_gain: float32 [4096], replicated, may hold values from 0.1 to 1.9
- expert_pick: int32 [8192, 2], P('ep'), may hold values from 0 to 31, as said below
- route_weight: float32 [8192, 2], P('ep'), may hold values from 0.2 to 1
- gate_weight: bfloat16 [32, 4096, 2048], P('ep', None, 'tp'), may hold values from -0.09375 to 0.09375
- up_weight: bfloat16 [32, 4096, 2048], P('ep', None, 'tp'), may hold values from -0.09375 to 0.09375
- down_weight: bfloat16 [32, 2048, 4096], P('ep', 'tp'), may hold values from -0.125 to 0.125
- post_gain: float32 [4096], replicated, may hold values from 0.1 to 1.9
Outputs:
- mixed_heads: bfloat16 [32768, 4096], P('ep', 'tp')
- routed_out: bfloat16 [8192, 4096], P(('ep', 'tp'))
The draws below stay inside these ranges and needn't reach their ends.
Inputs may be any that keep to these rules, and one draw needn't show every extreme that they name: `expert_pick`: each row names 2 different experts, both in the same one of 4 equal groups of consecutive expert numbers. In every aligned block of 32 rows no expert is named more than 4 times, and some expert exactly 4 times.
All inputs are finite; a program needn't handle non-finite values.
Results may differ from the reference program's by a relative error of at most 0.015.
Values may be sent and summed in bfloat16 or wider, within the bound.
A program may use at most 128 MiB of HBM per device.

```python
import math
import jax
import jax.numpy as jnp
from jax import lax

D = 4096
HEADS = 16
DK = 128
DV = 256
FF = 2048
GROUPS = 4
TOP_K = 2
BLK = 64
TOK_A_DEV = 1024
SPAN_LENGTH = 32768
TOK_B = 8192
EXPERTS = 32
PART_ROWS = 32
CAP = 4
N_EP = 32
N_TP = 8


def draw_decay_logit(key, part):
    channel_count = HEADS * DK
    random_subkeys = jax.random.split(jax.random.fold_in(key, 7), 7)
    slow_level = jnp.log(SPAN_LENGTH * 1.18 / 8.0)
    fast_share = 0.5
    jitter = jax.random.uniform(random_subkeys[0], (SPAN_LENGTH, channel_count), jnp.float32, -1.0, 1.0)
    fast_mask = jax.random.uniform(random_subkeys[1], (channel_count,), jnp.float32) < fast_share
    fast_level = jax.random.uniform(random_subkeys[2], (channel_count,), jnp.float32, 0.5, 1.5)
    slow_spread = jax.random.uniform(random_subkeys[3], (channel_count,), jnp.float32, -0.5, 0.5)
    baseline = jnp.where(fast_mask, fast_level, slow_level + slow_spread)
    shards = SPAN_LENGTH // TOK_A_DEV
    shifts = jax.random.uniform(random_subkeys[4], (shards,), jnp.float32, -0.7, 0.7)
    shift_rows = jnp.repeat(shifts, TOK_A_DEV)
    surge_rows = jax.random.randint(random_subkeys[5], (3,), 0, SPAN_LENGTH)
    surge_value = jax.random.uniform(random_subkeys[6], (3, channel_count), jnp.float32, -11.0, -3.5)
    dropped_indicator = (jnp.arange(SPAN_LENGTH)[:, None] == surge_rows[None, :]).astype(jnp.float32)
    spike_segment = jnp.dot(dropped_indicator, surge_value, precision=lax.Precision.HIGHEST)
    spike_exists = jnp.sum(dropped_indicator, axis=1, keepdims=True) > 0.0
    expert_affinity_scores = baseline[None, :] + jitter + shift_rows[:, None]
    expert_affinity_scores = jnp.where(spike_exists, spike_segment, expert_affinity_scores)
    return jnp.clip(expert_affinity_scores, -11.0, 16.0).astype(jnp.float32)


def pick_block(block_key):
    per_group = EXPERTS // GROUPS
    half_cap = CAP // 2
    random_subkeys = jax.random.split(block_key, 6)
    orders = jax.vmap(lambda one_key: jax.random.permutation(one_key, per_group))(jax.random.split(random_subkeys[0], GROUPS))
    orders = orders.astype(jnp.int32)
    inverse = jnp.argsort(orders, axis=1).astype(jnp.int32)
    offsets = jax.random.randint(random_subkeys[1], (GROUPS, 1), 1, per_group)
    opening_round = jnp.take_along_axis(orders, (inverse + 1) % per_group, axis=1)
    second_turn = jnp.take_along_axis(orders, (inverse + offsets) % per_group, axis=1)
    member = jnp.arange(per_group, dtype=jnp.int32)[None, :, None]
    copy_index = jnp.arange(half_cap, dtype=jnp.int32)[None, None, :]
    partner = jnp.where(copy_index % 2 == 0, opening_round[:, :, None], second_turn[:, :, None])
    group_base = (jnp.arange(GROUPS, dtype=jnp.int32) * per_group)[:, None, None]
    leader = jnp.broadcast_to(group_base + member, partner.shape).reshape(-1)
    follower = (group_base + partner).reshape(-1)
    pair_count = leader.shape[0]
    chosen = jax.random.randint(random_subkeys[2], (), 0, EXPERTS)
    forced = ((leader == chosen) | (follower == chosen)).astype(jnp.int32)
    ranks = jax.random.permutation(random_subkeys[3], pair_count).astype(jnp.int32)
    picked = jnp.argsort(-(ranks + forced * pair_count))[:PART_ROWS]
    picked = picked[jax.random.permutation(random_subkeys[4], PART_ROWS)]
    flips = jax.random.randint(random_subkeys[5], (PART_ROWS,), 0, 2)
    first_col = jnp.where(flips == 1, follower[picked], leader[picked])
    second_col = jnp.where(flips == 1, leader[picked], follower[picked])
    return jnp.stack([first_col, second_col], axis=1).astype(jnp.int32)


def draw_expert_pick(key, part):
    blocks = TOK_B // PART_ROWS
    block_keys = jax.random.split(jax.random.fold_in(key, 11), blocks)
    return jax.vmap(pick_block)(block_keys).reshape(TOK_B, TOP_K).astype(jnp.int32)


def block_scale(stream_key, extent, cuts, least, top_value):
    def one(dim, shards_of):
        steps = jax.random.uniform(jax.random.fold_in(jax.random.fold_in(stream_key, 6), dim), (shards_of,), jnp.float32, least / len(cuts), top_value / len(cuts))
        return jnp.repeat(jnp.exp(steps), extent[dim] // shards_of).reshape((-1,) + (1,) * (len(extent) - dim - 1))

    loudness = one(*cuts[0])
    for cut in cuts[1:]:
        loudness = loudness * one(*cut)
    return loudness


def bell_draw(own_key, dims, deviation, reach, pieces=(), kind=jnp.bfloat16):
    factor_of = block_scale(own_key, dims, pieces, -0.22, 0.18) if pieces else 1.0
    drawn = jax.random.normal(own_key, dims, jnp.float32) * deviation * factor_of
    return jnp.minimum(jnp.maximum(drawn, -reach), reach).astype(kind)


def setup_inputs(seed: int = 0) -> dict:
    streams_of = jax.random.split(jax.random.key(seed), 14)
    return {
        "queries": bell_draw(streams_of[0], (SPAN_LENGTH, HEADS * DK), 1.0, 6.0, ((0, 32), (1, 8))),
        "key_vectors": bell_draw(streams_of[1], (SPAN_LENGTH, HEADS * DK), 1.0, 6.0, ((0, 32), (1, 8))),
        "value_vectors": bell_draw(streams_of[2], (SPAN_LENGTH, HEADS * DV), 1.0, 6.0, ((0, 32), (1, 8))),
        "decay_logit": draw_decay_logit(jax.random.fold_in(streams_of[13], 71), 0),
        "head_gain": jnp.clip(1.0 + 0.18 * jax.random.normal(streams_of[4], (DV,), jnp.float32), 0.1, 1.9),
        "routed_rows": bell_draw(streams_of[5], (TOK_B, D), 1.0, 6.0, ((0, 32),)),
        "pre_gain": jnp.clip(1.0 + 0.18 * jax.random.normal(streams_of[6], (D,), jnp.float32), 0.1, 1.9),
        "expert_pick": draw_expert_pick(jax.random.fold_in(streams_of[13], 71), 0),
        "route_weight": jnp.clip(jnp.exp(math.log(1.0) - 1.609438 * jax.random.uniform(streams_of[8], (TOK_B, TOP_K), jnp.float32) ** block_scale(streams_of[8], (TOK_B, TOP_K), ((0, 32),), -0.2, 0.2)), 0.2, 1.0),
        "gate_weight": bell_draw(streams_of[9], (EXPERTS, D, FF), D ** -0.5, 0.09375, ((0, 32), (2, 8))),
        "up_weight": bell_draw(streams_of[10], (EXPERTS, D, FF), D ** -0.5, 0.09375, ((0, 32), (2, 8))),
        "down_weight": bell_draw(streams_of[11], (EXPERTS, FF, D), FF ** -0.5, 0.125, ((0, 32), (1, 8))),
        "post_gain": jnp.clip(1.0 + 0.18 * jax.random.normal(streams_of[12], (D,), jnp.float32), 0.1, 1.9),
    }


def to_half(array):
    return lax.optimization_barrier(array.astype(jnp.bfloat16))

def row_norm(values, gain):
    return values * lax.rsqrt(lax.optimization_barrier(jnp.mean(values * values, axis=-1, keepdims=True)) + 1e-06) * gain

def token_mixer(queries, key_vectors, value_vectors, decay_logit, head_gain):
    blocks = SPAN_LENGTH // BLK
    key_shape = (blocks, BLK, HEADS, DK)
    log_rate = (jax.nn.log_sigmoid(decay_logit) / 16.0).reshape(key_shape)
    query_blocks = queries.reshape(key_shape)
    key_blocks = key_vectors.reshape(key_shape)
    value_blocks = value_vectors.reshape(blocks, BLK, HEADS, DV)
    causal_mask = jnp.tril(jnp.ones((BLK, BLK), dtype=bool))

    def advance(carry_state, inputs):
        query_rows, key_rows, value_rows, rate_rows = inputs
        cumulative = jnp.cumsum(rate_rows, axis=0)
        ending = cumulative[-1]
        query_decay = to_half(query_rows.astype(jnp.float32) * jnp.exp(cumulative))
        key_decay = to_half(key_rows.astype(jnp.float32) * jnp.exp(-cumulative))
        key_to_end = to_half(key_rows.astype(jnp.float32) * jnp.exp(ending[None] - cumulative))
        values_wide = value_rows.astype(jnp.float32)
        scores = jnp.einsum('ihd,jhd->hij', query_decay.astype(jnp.float32), key_decay.astype(jnp.float32))
        weights = to_half(jnp.where(causal_mask[None], scores, 0.0))
        inside = jnp.einsum('hij,jhe->ihe', weights.astype(jnp.float32), values_wide)
        state_half = to_half(carry_state).astype(jnp.float32)
        carried = jnp.einsum('ihd,hde->ihe', query_decay.astype(jnp.float32), state_half)
        update = jnp.einsum('jhd,jhe->hde', key_to_end.astype(jnp.float32), values_wide)
        next_state = carry_state * jnp.exp(ending)[:, :, None] + update
        produced = row_norm(inside + carried, head_gain).astype(jnp.bfloat16)
        return (next_state, produced)
    start_state = jnp.zeros((HEADS, DK, DV), jnp.float32)
    _, outputs = lax.scan(advance, start_state, (query_blocks, key_blocks, value_blocks, log_rate))
    return outputs.reshape(SPAN_LENGTH, HEADS * DV)

def routed_experts(routed_rows, pre_gain, expert_pick, route_weight, gate_weight, up_weight, down_weight, post_gain):
    normed = row_norm(routed_rows.astype(jnp.float32), pre_gain).astype(jnp.bfloat16)
    flat_pick = expert_pick.reshape(-1).astype(jnp.int32)
    flat_weight = route_weight.reshape(-1)
    expert_room = N_EP * N_TP * CAP
    slice_width = FF // N_TP

    def per_expert(summed, expert):
        ordering = jnp.argsort((flat_pick != expert).astype(jnp.int32), stable=True)[:expert_room].astype(jnp.int32)
        is_live = flat_pick[ordering] == expert
        row_index = (ordering // TOP_K).astype(jnp.int32)
        inputs = normed[row_index].astype(jnp.float32)
        gate_act = jnp.dot(inputs, gate_weight[expert].astype(jnp.float32), preferred_element_type=jnp.float32)
        up_act = jnp.dot(inputs, up_weight[expert].astype(jnp.float32), preferred_element_type=jnp.float32)
        hidden = to_half(jax.nn.silu(gate_act) * up_act).astype(jnp.float32)
        running = jnp.zeros((expert_room, D), jnp.float32)
        for portion in range(N_TP):
            lower_edge = portion * slice_width
            partial_value = jnp.dot(hidden[:, lower_edge:lower_edge + slice_width], down_weight[expert, lower_edge:lower_edge + slice_width].astype(jnp.float32), preferred_element_type=jnp.float32)
            running = running + to_half(partial_value).astype(jnp.float32)
        produced = to_half(running).astype(jnp.float32)
        factor = jnp.where(is_live, flat_weight[ordering], jnp.zeros_like(flat_weight[ordering]))
        return (summed.at[row_index].add(factor[:, None] * produced), None)
    summed, _ = lax.scan(per_expert, jnp.zeros((TOK_B, D), jnp.float32), jnp.arange(EXPERTS, dtype=jnp.int32))
    return row_norm(summed, post_gain).astype(jnp.bfloat16)

def reference(queries, key_vectors, value_vectors, decay_logit, head_gain, routed_rows, pre_gain, expert_pick, route_weight, gate_weight, up_weight, down_weight, post_gain):
    mixed_heads = token_mixer(queries, key_vectors, value_vectors, decay_logit, head_gain)
    routed_out = routed_experts(routed_rows, pre_gain, expert_pick, route_weight, gate_weight, up_weight, down_weight, post_gain)
    return (mixed_heads, routed_out)
```

```python
import jax
import jax.numpy as jnp
from jax import lax
from jax.experimental import pallas as pl
from jax.experimental.pallas import tpu as pltpu
from jax.sharding import Mesh
from jax.sharding import PartitionSpec as P

BLK, DK, DV = 64, 128, 256
NZ, NX, NY = 8, 4, 4
D = 4096
MESH = pl.DeviceIdType.MESH
EP, TP = ("z", "x"), ("y", "c")
F32, BF16 = jnp.float32, jnp.bfloat16
VLIM = 60 * 1024 * 1024
NT = (((1,), (1,)), ((), ()))
TN = (((0,), (0,)), ((), ()))


def where_am_i():
    return tuple(lax.axis_index(a) for a in ("z", "x", "y", "c"))


def near(z, j):
    off = jnp.where(lax.rem(j, 2) == 1, (j + 1) // 2, NZ - j // 2)
    return lax.rem(z + off, NZ)


def remote(src, dst, ssem, rsem, **to):
    return pltpu.make_async_remote_copy(
        src_ref=src, dst_ref=dst, send_sem=ssem, recv_sem=rsem, device_id=to, device_id_type=MESH
    )


def await_bytes(ref, sem):
    pltpu.make_async_copy(ref, ref, sem).wait()


def greet(groups):
    barrier = pltpu.get_barrier_semaphore()
    total = 0
    for to, is_other in groups:
        if is_other is True:
            pl.semaphore_signal(barrier, inc=1, device_id=to, device_id_type=MESH)
            total = total + 1
        else:

            @pl.when(is_other)
            def _(to=to):
                pl.semaphore_signal(barrier, inc=1, device_id=to, device_id_type=MESH)

            total = total + is_other.astype(jnp.int32)
    pl.semaphore_wait(barrier, total)


def exchange_peers(z, x, y, c):
    peers = []
    for dz in range(NZ):
        for xh in range(2):
            zd, xd = lax.rem(z + dz, NZ), 2 * xh + c
            to = {"z": zd, "x": xd, "y": y, "c": lax.rem(x, 2)}
            peers.append((to, True if dz else jnp.logical_not((xd == x) & (lax.rem(x, 2) == c))))
    return peers


def tp_peers(y, c):
    return [
        ({"y": lax.rem(y + 1, NY)}, True),
        ({"y": lax.rem(y + NY - 1, NY)}, True),
        ({"c": 1 - c}, True),
    ]


def slot_matrix(picks, c):
    shape = (2 * 32, 128)
    r = lax.broadcasted_iota(jnp.int32, shape, 0)
    i = lax.broadcasted_iota(jnp.int32, shape, 1)
    expert = 2 * (i >> 3) + c
    same_block = (r >> 5) == ((i >> 2) & 1)
    first = (picks[:, 0:1] == expert) & same_block
    second = (picks[:, 1:2] == expert) & same_block
    named = jnp.where(first | second, 1.0, 0.0).astype(BF16)
    rr = lax.broadcasted_iota(jnp.int32, (64, 64), 0)
    cc = lax.broadcasted_iota(jnp.int32, (64, 64), 1)
    earlier = jnp.where(cc < rr, 1.0, 0.0).astype(BF16)
    rank = jnp.dot(earlier, named, preferred_element_type=F32)
    fits = rank == (i & 3).astype(F32)
    return first & fits, second & fits


def prep_body(rows_hbm, picks_ref, weight_ref, gain_ref, out_ref, w_ref, rows, sem):
    _, _, y, c = where_am_i()
    copy = pltpu.make_async_copy(rows_hbm.at[pl.ds(y * 64, 64)], rows, sem)
    copy.start()
    first, second = slot_matrix(picks_ref[...], c)
    weights = weight_ref[...]
    w_ref[...] = jnp.where(first, weights[:, 0:1], 0.0) + jnp.where(second, weights[:, 1:2], 0.0)
    select = jnp.where(first | second, 1.0, 0.0).astype(BF16)
    copy.wait()
    wide = rows[...].astype(F32)
    scale = lax.rsqrt(jnp.mean(wide * wide, axis=-1, keepdims=True) + 1e-6)
    step = 512
    for n in range(0, D, step):
        normed = (wide[:, n : n + step] * scale * gain_ref[:, n : n + step]).astype(BF16)
        got = lax.dot_general(select, normed, TN, preferred_element_type=F32)
        out_ref[:, :, n : n + step] = got.reshape(16, 8, step).astype(BF16)


def prep(rows, picks, weights, gain):
    return pl.pallas_call(
        prep_body,
        out_shape=(jax.ShapeDtypeStruct((16, 8, D), BF16), jax.ShapeDtypeStruct((64, 128), F32)),
        in_specs=[pl.BlockSpec(memory_space=pl.ANY)] + [pl.BlockSpec(memory_space=pltpu.VMEM)] * 3,
        out_specs=[pl.BlockSpec(memory_space=pltpu.VMEM)] * 2,
        scratch_shapes=[pltpu.VMEM((64, D), BF16), pltpu.SemaphoreType.DMA],
        compiler_params=pltpu.CompilerParams(vmem_limit_bytes=VLIM),
        name="prep",
    )(rows, picks, weights, gain)


def rates(logit):
    rate = (jnp.minimum(logit, 0.0) - jnp.log1p(jnp.exp(-jnp.abs(logit)))) * (1.0 / 16.0)
    hi = rate.astype(BF16)
    rest = rate - hi.astype(F32)
    mid = rest.astype(BF16)
    low = (rest - mid.astype(F32)).astype(BF16)
    rr = lax.broadcasted_iota(jnp.int32, (BLK, BLK), 0)
    cc = lax.broadcasted_iota(jnp.int32, (BLK, BLK), 1)
    lower = jnp.where(cc <= rr, 1.0, 0.0).astype(BF16)
    cum = jnp.dot(lower, low, preferred_element_type=F32)
    cum = cum + jnp.dot(lower, mid, preferred_element_type=F32)
    return cum + jnp.dot(lower, hi, preferred_element_type=F32)


def pass_a(k_ref, v_ref, g_ref, st_ref, tot_ref):
    st_ref[...] = jnp.zeros_like(st_ref)
    tot_ref[...] = jnp.zeros_like(tot_ref)

    def block(n, carry):
        at = pl.ds(n * BLK, BLK)
        cum = rates(g_ref[at, :])
        end = cum[BLK - 1 : BLK, :]
        to_end = (k_ref[at, :].astype(F32) * jnp.exp(end - cum)).astype(BF16)
        decay = jnp.exp(end)
        values = v_ref[at, :]
        for h in range(2):
            update = lax.dot_general(
                values[:, h * DV : (h + 1) * DV],
                to_end[:, h * DK : (h + 1) * DK],
                TN,
                preferred_element_type=F32,
            )
            st_ref[h] = st_ref[h] * decay[:, h * DK : (h + 1) * DK] + update
        tot_ref[...] = tot_ref[...] + end
        return carry

    lax.fori_loop(0, 16, block, 0)


def pass_b_block(n, q_ref, k_ref, v_ref, g_ref, gain_ref, st_ref, out_ref):
    at = pl.ds(pl.multiple_of(n * BLK, BLK), BLK)
    cum = rates(g_ref[at, :])
    end = cum[BLK - 1 : BLK, :]
    keys = k_ref[at, :].astype(F32)
    query_decay = (q_ref[at, :].astype(F32) * jnp.exp(cum)).astype(BF16)
    key_decay = (keys * jnp.exp(-cum)).astype(BF16)
    to_end = (keys * jnp.exp(end - cum)).astype(BF16)
    decay = jnp.exp(end)
    values = v_ref[at, :]
    rr = lax.broadcasted_iota(jnp.int32, (BLK, BLK), 0)
    cc = lax.broadcasted_iota(jnp.int32, (BLK, BLK), 1)
    for h in range(2):
        ks, vs = slice(h * DK, (h + 1) * DK), slice(h * DV, (h + 1) * DV)
        scores = lax.dot_general(query_decay[:, ks], key_decay[:, ks], NT, preferred_element_type=F32)
        weights = jnp.where(cc <= rr, scores, 0.0).astype(BF16)
        state = st_ref[h]
        total = jnp.dot(weights, values[:, vs], preferred_element_type=F32) + lax.dot_general(
            query_decay[:, ks], state.astype(BF16), NT, preferred_element_type=F32
        )
        scale = lax.rsqrt(jnp.mean(total * total, axis=-1, keepdims=True) + 1e-6)
        out_ref[at, vs] = (total * scale * gain_ref[...]).astype(BF16)
        update = lax.dot_general(values[:, vs], to_end[:, ks], TN, preferred_element_type=F32)
        st_ref[h] = state * decay[:, ks] + update


def k1_body(
    out_hbm, k_ref, v_ref, g_ref, arr, inc,
    st, tot, xs, xr, zs_buf, zr, acc, pbuf,
    a_send, a_recv, y_send, y_recv, f_send, p_send, p_recv,
    x1_send, x1_recv, z_send, z_recv, x2_send, x2_recv,
):
    z, x, y, c = where_am_i()
    up, down, far = lax.rem(y + 1, NY), lax.rem(y + NY - 1, NY), lax.rem(y + 2, NY)
    xpar, xhalf = lax.rem(x, 2), x // 2
    groups = exchange_peers(z, x, y, c) + tp_peers(y, c)
    groups += [({"x": lax.rem(x + d, NX)}, True) for d in range(1, NX)]
    groups += [({"z": lax.rem(z + d, NZ)}, True) for d in range(1, NZ)]
    greet(groups)

    def is_self(zd, xd):
        return (zd == z) & (xd == x) & (xpar == c)

    def exchange(j, xh):
        zd, xd = near(z, j), 2 * xh + c
        return is_self(zd, xd), remote(
            out_hbm.at[zd * 2 + xh],
            arr.at[xpar, y, z, xhalf],
            a_send.at[zd, xh],
            a_recv.at[z],
            z=zd,
            x=xd,
            y=y,
            c=xpar,
        )

    def send_out(j, carry):
        for xh in range(2):
            own, copy = exchange(j, xh)

            @pl.when(own)
            def _():
                pltpu.make_async_copy(out_hbm.at[z * 2 + xhalf], arr.at[c, y, z, xhalf], a_recv.at[z]).start()

            @pl.when(jnp.logical_not(own))
            def _():
                copy.start()

        return carry

    lax.fori_loop(0, NZ, send_out, 0)

    pass_a(k_ref, v_ref, g_ref, st, tot)
    dec = jnp.exp(tot[...])
    for h in range(2):
        row = jnp.broadcast_to(dec[:, h * DK : (h + 1) * DK], (8, DK))
        hi = row.astype(BF16)
        low = (row - hi.astype(F32)).astype(BF16)
        for part in range(4):
            xs[part, h, 0:64, :] = st[h, part * 64 : (part + 1) * 64, :].astype(BF16)
            xs[part, h, 64:72, :] = hi
            xs[part, h, 72:80, :] = low
    xr[x] = xs[x]

    def x1(d):
        xd = lax.rem(x + d, NX)
        return remote(xs.at[xd], xr.at[x], x1_send.at[d - 1], x1_recv.at[x], x=xd)

    for d in range(1, NX):
        x1(d).start()

    def own_copies(j):
        s = near(z, j)
        piece = arr.at[c, y, s]
        return [
            remote(piece, piece, y_send.at[0, s], y_recv.at[y, s], y=up),
            remote(piece, piece, y_send.at[1, s], y_recv.at[y, s], y=down),
            remote(piece, piece, p_send.at[y, s], p_recv.at[y, s], c=1 - c),
        ]

    def to_partner(ysrc, s):
        piece = arr.at[c, ysrc, s]
        return remote(piece, piece, p_send.at[ysrc, s], p_recv.at[ysrc, s], c=1 - c)

    def onward(ysrc, s, ydst):
        piece = arr.at[c, ysrc, s]
        return remote(piece, piece, f_send.at[s], y_recv.at[ysrc, s], y=ydst)

    def gather_step(i, carry):
        @pl.when(i < NZ)
        def _():
            s = near(z, i)
            await_bytes(arr.at[c, y, s], a_recv.at[s])
            for copy in own_copies(i):
                copy.start()

        @pl.when((i >= 1) & (i < NZ + 1))
        def _():
            j = i - 1
            s = near(z, j)
            await_bytes(arr.at[c, down, s], y_recv.at[down, s])

            @pl.when(lax.rem(j, 2) == 0)
            def _():
                onward(down, s, up).start()

            to_partner(down, s).start()
            await_bytes(arr.at[c, up, s], y_recv.at[up, s])

            @pl.when(lax.rem(j, 2) == 1)
            def _():
                onward(up, s, down).start()

            to_partner(up, s).start()

        @pl.when(i >= 2)
        def _():
            s = near(z, i - 2)
            await_bytes(arr.at[c, far, s], y_recv.at[far, s])
            to_partner(far, s).start()

        return carry

    lax.fori_loop(0, 6, gather_step, 0)

    for d in range(1, NX):
        src = lax.rem(x + d, NX)
        await_bytes(xr.at[src], x1_recv.at[src])

    def part_of(buf, at, h):
        piece = buf[at, h].astype(F32)
        return piece[0:64, :], piece[64:65, :] + piece[72:73, :]

    for h in range(2):
        state, decay = part_of(xr, 0, h)
        for k in range(1, NX):
            s_k, d_k = part_of(xr, k, h)
            state = state * d_k + s_k
            decay = decay * d_k
        row = jnp.broadcast_to(decay, (8, DK))
        hi = row.astype(BF16)
        zs_buf[h, 0:64, :] = state.astype(BF16)
        zs_buf[h, 64:72, :] = hi
        zs_buf[h, 72:80, :] = (row - hi.astype(F32)).astype(BF16)

    def z_copy(zd):
        return remote(zs_buf, zr.at[z], z_send.at[zd], z_recv.at[z], z=zd)

    for zd in range(1, NZ):

        @pl.when(zd > z)
        def _(zd=zd):
            z_copy(zd).start()

    lax.fori_loop(6, NZ + 2, gather_step, 0)

    acc[...] = jnp.zeros_like(acc)
    for zsrc in range(NZ - 1):

        @pl.when(zsrc < z)
        def _(zsrc=zsrc):
            await_bytes(zr.at[zsrc], z_recv.at[zsrc])
            for h in range(2):
                s_k, d_k = part_of(zr, zsrc, h)
                acc[h] = acc[h] * d_k + s_k

    for h in range(2):
        state = acc[h]
        for k in range(NX):
            pbuf[k, h] = state
            s_k, d_k = part_of(xr, k, h)
            state = state * d_k + s_k
    inc[x] = pbuf[x]

    def x2(d):
        xd = lax.rem(x + d, NX)
        return remote(pbuf.at[xd], inc.at[x], x2_send.at[d - 1], x2_recv.at[x], x=xd)

    for d in range(1, NX):
        x2(d).start()

    def finish(j, carry):
        for xh in range(2):
            own, copy = exchange(j, xh)

            @pl.when(jnp.logical_not(own))
            def _():
                copy.wait_send()

        s = near(z, j)
        for copy in own_copies(j)[:2]:
            copy.wait_send()

        @pl.when(lax.rem(j, 2) == 0)
        def _():
            onward(down, s, up).wait_send()

        @pl.when(lax.rem(j, 2) == 1)
        def _():
            onward(up, s, down).wait_send()

        for ysrc in range(NY):
            to_partner(ysrc, s).wait_send()
            await_bytes(arr.at[1 - c, ysrc, s], p_recv.at[ysrc, s])
        return carry

    lax.fori_loop(0, NZ, finish, 0)
    for zd in range(1, NZ):

        @pl.when(zd > z)
        def _(zd=zd):
            z_copy(zd).wait_send()

    for d in range(1, NX):
        x1(d).wait_send()
        x2(d).wait_send()
        src = lax.rem(x + d, NX)
        await_bytes(inc.at[src], x2_recv.at[src])


def k1(outgoing, k, v, g):
    dma = pltpu.SemaphoreType.DMA
    vmem = pl.BlockSpec(memory_space=pltpu.VMEM)
    return pl.pallas_call(
        k1_body,
        out_shape=(
            jax.ShapeDtypeStruct((2, NY, NZ, 2, 8, D), BF16),
            jax.ShapeDtypeStruct((4, 2, 64, DK), F32),
        ),
        in_specs=[pl.BlockSpec(memory_space=pl.ANY), vmem, vmem, vmem],
        out_specs=[vmem, vmem],
        scratch_shapes=[
            pltpu.VMEM((2, DV, DK), F32),
            pltpu.VMEM((1, 2 * DK), F32),
            pltpu.VMEM((4, 2, 80, DK), BF16),
            pltpu.VMEM((4, 2, 80, DK), BF16),
            pltpu.VMEM((2, 80, DK), BF16),
            pltpu.VMEM((NZ, 2, 80, DK), BF16),
            pltpu.VMEM((2, 64, DK), F32),
            pltpu.VMEM((4, 2, 64, DK), F32),
            dma((NZ, 2)), dma((NZ,)), dma((2, NZ)), dma((NY, NZ)), dma((NZ,)), dma((NY, NZ)), dma((NY, NZ)),
            dma((3,)), dma((4,)), dma((NZ,)), dma((NZ,)), dma((3,)), dma((4,)),
        ],
        compiler_params=pltpu.CompilerParams(collective_id=0, has_side_effects=True, vmem_limit_bytes=VLIM),
        name="dispatch",
    )(outgoing, k, v, g)


def ffn_body(x_ref, gate_ref, up_ref, down_ref, o_ref):
    rows = x_ref[...]
    gate = jnp.dot(rows, gate_ref[...], preferred_element_type=F32)
    up = jnp.dot(rows, up_ref[...], preferred_element_type=F32)
    hidden = (gate / (1.0 + jnp.exp(-gate)) * up).astype(BF16)
    step = 1024
    for n in range(0, D, step):
        o_ref[:, n : n + step] = jnp.dot(
            hidden, down_ref[:, n : n + step], preferred_element_type=F32
        ).astype(BF16)


def ffn(rows, gate, up, down):
    tile = 256
    width = gate.shape[1]
    return pl.pallas_call(
        ffn_body,
        grid=(rows.shape[0] // tile,),
        out_shape=jax.ShapeDtypeStruct(rows.shape, BF16),
        in_specs=[
            pl.BlockSpec((tile, D), lambda i: (i, 0)),
            pl.BlockSpec((D, width), lambda i: (0, 0)),
            pl.BlockSpec((D, width), lambda i: (0, 0)),
            pl.BlockSpec((width, D), lambda i: (0, 0)),
        ],
        out_specs=pl.BlockSpec((tile, D), lambda i: (i, 0)),
        compiler_params=pltpu.CompilerParams(vmem_limit_bytes=VLIM),
        name="expert",
    )(rows, gate, up, down)


def k3_body(
    part, w_ref, post_ref, q_ref, k_ref, v_ref, g_ref, gain_ref, inc_ref, mixed, routed,
    r1, low, upd, fin, ret, st, mine, cs, cr,
    d_send, d_recv, l_send, l_recv, t_send, u_send, u_recv, b_send, b_recv, c_send, c_recv,
):
    z, x, y, c = where_am_i()
    up, down, far = lax.rem(y + 1, NY), lax.rem(y + NY - 1, NY), lax.rem(y + 2, NY)
    xpar, xhalf = lax.rem(x, 2), x // 2
    greet(exchange_peers(z, x, y, c) + tp_peers(y, c))

    def over(j):
        s = near(z, j)
        return remote(part.at[1 - c, :, s], r1.at[:, s], d_send.at[s], d_recv.at[s], c=1 - c)

    def start_over(j, carry):
        over(j).start()
        return carry

    lax.fori_loop(0, NZ, start_over, 0)

    for h in range(2):
        for part_no in range(4):
            st[h, part_no * 64 : (part_no + 1) * 64, :] = inc_ref[part_no, h]

    def relay(j, to):
        s = near(z, j)
        return remote(r1.at[far, s], low.at[s], l_send.at[s], l_recv.at[s], y=to)

    def direct(j, to, side):
        s = near(z, j)
        return remote(r1.at[to, s], upd.at[side, s], u_send.at[s], u_recv.at[side, s], y=to)

    def joined(j, to, side):
        s = near(z, j)
        return remote(r1.at[to, s], upd.at[side, s], t_send.at[s], u_recv.at[side, s], y=to)

    def back(j, xh):
        s = near(z, j)
        xd = 2 * xh + c
        own = (s == z) & (xd == x) & (xpar == c)
        return own, remote(
            fin.at[s, xh],
            ret.at[z, xhalf],
            b_send.at[s, xh],
            b_recv.at[z, xhalf],
            z=s,
            x=xd,
            y=y,
            c=xpar,
        )

    def step(i, carry):
        @pl.when(i < NZ)
        def _():
            j = i
            s = near(z, j)
            even = lax.rem(j, 2) == 0
            await_bytes(r1.at[:, s], d_recv.at[s])

            def add(yy, inner):
                for xh in range(2):
                    r1[yy, s, xh] = (r1[yy, s, xh].astype(F32) + part[c, yy, s, xh].astype(F32)).astype(BF16)
                return inner

            lax.fori_loop(0, NY, add, 0)

            @pl.when(even)
            def _():
                relay(j, down).start()
                direct(j, up, 0).start()

            @pl.when(jnp.logical_not(even))
            def _():
                relay(j, up).start()
                direct(j, down, 1).start()

            for half in range(2):
                pass_b_block(2 * i + half, q_ref, k_ref, v_ref, g_ref, gain_ref, st, mixed)

        @pl.when((i >= 1) & (i < NZ + 1))
        def _():
            j = i - 1
            s = near(z, j)
            even = lax.rem(j, 2) == 0
            await_bytes(low.at[s], l_recv.at[s])
            to = jnp.where(even, down, up)
            for xh in range(2):
                r1[to, s, xh] = (r1[to, s, xh].astype(F32) + low[s, xh].astype(F32)).astype(BF16)

            @pl.when(even)
            def _():
                joined(j, down, 1).start()

            @pl.when(jnp.logical_not(even))
            def _():
                joined(j, up, 0).start()

        @pl.when(i >= 2)
        def _():
            j = i - 2
            s = near(z, j)
            for side in range(2):
                await_bytes(upd.at[side, s], u_recv.at[side, s])
            for xh in range(2):
                total = r1[y, s, xh].astype(F32) + upd[0, s, xh].astype(F32) + upd[1, s, xh].astype(F32)
                fin[s, xh] = total.astype(BF16)
                own, copy = back(j, xh)

                @pl.when(own)
                def _(xh=xh):
                    ret[s, xh] = fin[s, xh]

                @pl.when(jnp.logical_not(own))
                def _(copy=copy):
                    copy.start()

        return carry

    lax.fori_loop(0, NZ + 2, step, 0)

    def finish(j, carry):
        s = near(z, j)
        for xh in range(2):
            own, copy = back(j, xh)

            @pl.when(jnp.logical_not(own))
            def _(copy=copy, xh=xh):
                copy.wait_send()
                await_bytes(ret.at[s, xh], b_recv.at[s, xh])

        over(j).wait_send()
        await_bytes(low.at[s], l_send.at[s])
        await_bytes(low.at[s], u_send.at[s])
        await_bytes(low.at[s], t_send.at[s])
        return carry

    lax.fori_loop(0, NZ, finish, 0)

    weights = w_ref[...]
    w_hi = weights.astype(BF16)
    w_low = (weights - w_hi.astype(F32)).astype(BF16)
    width = 512

    def weigh(n, carry):
        at = pl.ds(pl.multiple_of(n * width, width), width)
        rows = ret[:, :, :, at].astype(F32).reshape(128, width).astype(BF16)
        got = jnp.dot(w_hi, rows, preferred_element_type=F32) + jnp.dot(w_low, rows, preferred_element_type=F32)
        mine[:, at] = jnp.where(c == 0, got[0:32], got[32:64])
        cs[:, at] = jnp.where(c == 0, got[32:64], got[0:32])
        return carry

    lax.fori_loop(0, D // width, weigh, 0)
    swap = remote(cs, cr, c_send, c_recv, c=1 - c)
    swap.start()
    swap.wait()
    total = mine[...] + cr[...]
    scale = lax.rsqrt(jnp.mean(total * total, axis=-1, keepdims=True) + 1e-6)
    routed[...] = (total * scale * post_ref[...]).astype(BF16)


def k3(part, w, post, q, k, v, g, gain, inc):
    dma = pltpu.SemaphoreType.DMA
    vmem = pl.BlockSpec(memory_space=pltpu.VMEM)
    return pl.pallas_call(
        k3_body,
        out_shape=(
            jax.ShapeDtypeStruct((1024, 2 * DV), BF16),
            jax.ShapeDtypeStruct((32, D), BF16),
        ),
        in_specs=[vmem] * 9,
        out_specs=[vmem, vmem],
        scratch_shapes=[
            pltpu.VMEM((NY, NZ, 2, 8, D), BF16),
            pltpu.VMEM((NZ, 2, 8, D), BF16),
            pltpu.VMEM((2, NZ, 2, 8, D), BF16),
            pltpu.VMEM((NZ, 2, 8, D), BF16),
            pltpu.VMEM((NZ, 2, 8, D), BF16),
            pltpu.VMEM((2, DV, DK), F32),
            pltpu.VMEM((32, D), F32),
            pltpu.VMEM((32, D), F32),
            pltpu.VMEM((32, D), F32),
            dma((NZ,)), dma((NZ,)), dma((NZ,)), dma((NZ,)), dma((NZ,)), dma((NZ,)), dma((2, NZ)),
            dma((NZ, 2)), dma((NZ, 2)), dma(()), dma(()),
        ],
        compiler_params=pltpu.CompilerParams(collective_id=1, has_side_effects=True, vmem_limit_bytes=VLIM),
        name="combine",
    )(part, w, post, q, k, v, g, gain, inc)


def on_device(
    queries,
    key_vectors,
    value_vectors,
    decay_logit,
    head_gain,
    routed_rows,
    pre_gain,
    expert_pick,
    route_weight,
    gate_weight,
    up_weight,
    down_weight,
    post_gain,
):
    y = lax.axis_index("y")
    picks = lax.dynamic_slice_in_dim(expert_pick, y * 64, 64, 0)
    weights = lax.dynamic_slice_in_dim(route_weight, y * 64, 64, 0)
    outgoing, w = prep(routed_rows, picks, weights, pre_gain.reshape(1, D))
    arrived, incoming = k1(outgoing, key_vectors, value_vectors, decay_logit)
    part = ffn(arrived.reshape(1024, D), gate_weight[0], up_weight[0], down_weight[0])
    return k3(
        part.reshape(arrived.shape),
        w,
        post_gain.reshape(1, D),
        queries,
        key_vectors,
        value_vectors,
        decay_logit,
        head_gain.reshape(1, DV),
        incoming,
    )


def solution(mesh):
    torus = Mesh(mesh.devices.reshape(NZ, NX, NY, 2), ("z", "x", "y", "c"))
    placed = (
        P(EP, TP),
        P(EP, TP),
        P(EP, TP),
        P(EP, TP),
        P(),
        P(EP, None),
        P(),
        P(EP, None),
        P(EP, None),
        P(EP, None, TP),
        P(EP, None, TP),
        P(EP, TP, None),
        P(),
    )
    return jax.shard_map(
        on_device,
        mesh=torus,
        in_specs=placed,
        out_specs=(P(EP, TP), P(EP + TP, None)),
        check_vma=False,
    )
```

```python
import jax
import jax.numpy as jnp
from jax import lax
from jax.experimental import pallas as pl
from jax.experimental.pallas import tpu as pltpu
from jax.sharding import Mesh
from jax.sharding import PartitionSpec as P

BLK, DK, DV = 64, 128, 256
NZ, NX, NY = 8, 4, 4
D = 4096
MESH = pl.DeviceIdType.MESH
EP, TP = ("z", "x"), ("y", "c")
F32, BF16 = jnp.float32, jnp.bfloat16
VLIM = 60 * 1024 * 1024
NT = (((1,), (1,)), ((), ()))
TN = (((0,), (0,)), ((), ()))


def where_am_i():
    return tuple(lax.axis_index(a) for a in ("z", "x", "y", "c"))


def near(z, j):
    off = jnp.where(lax.rem(j, 2) == 1, (j + 1) // 2, NZ - j // 2)
    return lax.rem(z + off, NZ)


def remote(src, dst, ssem, rsem, **to):
    return pltpu.make_async_remote_copy(
        src_ref=src, dst_ref=dst, send_sem=ssem, recv_sem=rsem, device_id=to, device_id_type=MESH
    )


def await_bytes(ref, sem):
    pltpu.make_async_copy(ref, ref, sem).wait()


def greet(groups):
    barrier = pltpu.get_barrier_semaphore()
    total = 0
    for to, is_other in groups:
        if is_other is True:
            pl.semaphore_signal(barrier, inc=1, device_id=to, device_id_type=MESH)
            total = total + 1
        else:

            @pl.when(is_other)
            def _(to=to):
                pl.semaphore_signal(barrier, inc=1, device_id=to, device_id_type=MESH)

            total = total + is_other.astype(jnp.int32)
    return barrier, total


def exchange_peers(z, x, y, c):
    peers = []
    for dz in range(NZ):
        for xh in range(2):
            zd, xd = lax.rem(z + dz, NZ), 2 * xh + c
            to = {"z": zd, "x": xd, "y": y, "c": lax.rem(x, 2)}
            peers.append((to, True if dz else jnp.logical_not((xd == x) & (lax.rem(x, 2) == c))))
    return peers


def tp_peers(y, c):
    return [
        ({"y": lax.rem(y + 1, NY)}, True),
        ({"y": lax.rem(y + NY - 1, NY)}, True),
        ({"c": 1 - c}, True),
    ]


def quarter(row, y):
    parts = [row[:, k * 64 : (k + 1) * 64] for k in range(4)]
    return jnp.where(y == 0, parts[0], jnp.where(y == 1, parts[1], jnp.where(y == 2, parts[2], parts[3])))


def slot_matrices(first_pick, second_pick, c):
    shape = (128, 64)
    i = lax.broadcasted_iota(jnp.int32, shape, 0)
    r = lax.broadcasted_iota(jnp.int32, shape, 1)
    expert = 2 * (i >> 3) + c
    same_block = (r >> 5) == ((i >> 2) & 1)
    first = (first_pick == expert) & same_block
    second = (second_pick == expert) & same_block
    named = jnp.where(first | second, 1.0, 0.0).astype(BF16)
    rr = lax.broadcasted_iota(jnp.int32, (64, 64), 0)
    cc = lax.broadcasted_iota(jnp.int32, (64, 64), 1)
    earlier = jnp.where(rr < cc, 1.0, 0.0).astype(BF16)
    rank = jnp.dot(named, earlier, preferred_element_type=F32)
    fits = rank == (i & 3).astype(F32)
    return first & fits, second & fits


def rates(logit):
    rate = (jnp.minimum(logit, 0.0) - jnp.log1p(jnp.exp(-jnp.abs(logit)))) * (1.0 / 16.0)
    hi = rate.astype(BF16)
    rest = rate - hi.astype(F32)
    mid = rest.astype(BF16)
    low = (rest - mid.astype(F32)).astype(BF16)
    rr = lax.broadcasted_iota(jnp.int32, (BLK, BLK), 0)
    cc = lax.broadcasted_iota(jnp.int32, (BLK, BLK), 1)
    lower = jnp.where(cc <= rr, 1.0, 0.0).astype(BF16)
    cum = jnp.dot(lower, low, preferred_element_type=F32)
    cum = cum + jnp.dot(lower, mid, preferred_element_type=F32)
    return cum + jnp.dot(lower, hi, preferred_element_type=F32)


def pass_a(k_ref, v_ref, g_ref, st_ref, tot_ref):
    st_ref[...] = jnp.zeros_like(st_ref)
    tot_ref[...] = jnp.zeros_like(tot_ref)

    def block(n, carry):
        at = pl.ds(n * BLK, BLK)
        cum = rates(g_ref[at, :])
        end = cum[BLK - 1 : BLK, :]
        to_end = (k_ref[at, :].astype(F32) * jnp.exp(end - cum)).astype(BF16)
        decay = jnp.exp(end)
        values = v_ref[at, :]
        for h in range(2):
            update = lax.dot_general(
                values[:, h * DV : (h + 1) * DV],
                to_end[:, h * DK : (h + 1) * DK],
                TN,
                preferred_element_type=F32,
            )
            st_ref[h] = st_ref[h] * decay[:, h * DK : (h + 1) * DK] + update
        tot_ref[...] = tot_ref[...] + end
        return carry

    lax.fori_loop(0, 16, block, 0)


def pass_b_block(n, q_ref, k_ref, v_ref, g_ref, gain_ref, st_ref, out_ref):
    at = pl.ds(pl.multiple_of(n * BLK, BLK), BLK)
    cum = rates(g_ref[at, :])
    end = cum[BLK - 1 : BLK, :]
    keys = k_ref[at, :].astype(F32)
    query_decay = (q_ref[at, :].astype(F32) * jnp.exp(cum)).astype(BF16)
    key_decay = (keys * jnp.exp(-cum)).astype(BF16)
    to_end = (keys * jnp.exp(end - cum)).astype(BF16)
    decay = jnp.exp(end)
    values = v_ref[at, :]
    rr = lax.broadcasted_iota(jnp.int32, (BLK, BLK), 0)
    cc = lax.broadcasted_iota(jnp.int32, (BLK, BLK), 1)
    for h in range(2):
        ks, vs = slice(h * DK, (h + 1) * DK), slice(h * DV, (h + 1) * DV)
        scores = lax.dot_general(query_decay[:, ks], key_decay[:, ks], NT, preferred_element_type=F32)
        weights = jnp.where(cc <= rr, scores, 0.0).astype(BF16)
        state = st_ref[h]
        total = jnp.dot(weights, values[:, vs], preferred_element_type=F32) + lax.dot_general(
            query_decay[:, ks], state.astype(BF16), NT, preferred_element_type=F32
        )
        scale = lax.rsqrt(jnp.mean(total * total, axis=-1, keepdims=True) + 1e-6)
        out_ref[at, vs] = (total * scale * gain_ref[...]).astype(BF16)
        update = lax.dot_general(values[:, vs], to_end[:, ks], TN, preferred_element_type=F32)
        st_ref[h] = state * decay[:, ks] + update


LAST = NZ + 6


def body(
    picks_ref, weight_ref, pre_ref, post_ref, gain_ref,
    rows_hbm, gate_hbm, up_hbm, down_hbm, q_hbm, k_hbm, v_hbm, g_hbm,
    mixed, routed,
    rows, gate_w, up_w, down_w, q_ref, k_ref, v_ref, g_ref,
    outgoing, w_buf, arr, xb, part, r1, low, upd, fin, ret, mine, cs, cr,
    st, tot, xs, xr, zs_buf, zr, acc, pbuf, inc,
    load, a_send, a_recv, y_send, y_recv, f_send, p_send, p_recv,
    x1_send, x1_recv, z_send, z_recv, x2_send, x2_recv,
    d_send, d_recv, l_send, l_recv, t_send, u_send, u_recv, b_send, b_recv, c_send, c_recv,
):
    z, x, y, c = where_am_i()
    up, down, far = lax.rem(y + 1, NY), lax.rem(y + NY - 1, NY), lax.rem(y + 2, NY)
    xpar, xhalf = lax.rem(x, 2), x // 2
    loads = [
        pltpu.make_async_copy(src, dst, load.at[n])
        for n, (src, dst) in enumerate(
            [
                (rows_hbm.at[pl.ds(y * 64, 64)], rows),
                (k_hbm, k_ref),
                (v_hbm, v_ref),
                (g_hbm, g_ref),
                (gate_hbm, gate_w),
                (up_hbm, up_w),
                (down_hbm, down_w),
                (q_hbm, q_ref),
            ]
        )
    ]
    for copy in loads:
        copy.start()
    groups = exchange_peers(z, x, y, c) + tp_peers(y, c)
    groups += [({"x": lax.rem(x + d, NX)}, True) for d in range(1, NX)]
    groups += [({"z": lax.rem(z + d, NZ)}, True) for d in range(1, NZ)]
    barrier, signals = greet(groups)

    first, second = slot_matrices(quarter(picks_ref[0:1, :], y), quarter(picks_ref[1:2, :], y), c)
    w_buf[...] = jnp.where(first, quarter(weight_ref[0:1, :], y), 0.0) + jnp.where(
        second, quarter(weight_ref[1:2, :], y), 0.0
    )
    select = jnp.where(first | second, 1.0, 0.0).astype(BF16)
    loads[0].wait()
    wide = rows[...].astype(F32)
    scale = lax.rsqrt(jnp.mean(wide * wide, axis=-1, keepdims=True) + 1e-6)
    width = 512
    for n in range(0, D, width):
        normed = (wide[:, n : n + width] * scale * pre_ref[:, n : n + width]).astype(BF16)
        got = jnp.dot(select, normed, preferred_element_type=F32)
        outgoing[:, :, n : n + width] = got.reshape(16, 8, width).astype(BF16)
    pl.semaphore_wait(barrier, signals)

    def piece(j, xh):
        s, xd = near(z, j), 2 * xh + c
        return (s == z) & (xd == x) & (xpar == c), s, xd

    def exchange(j, xh):
        own, s, xd = piece(j, xh)
        return own, remote(
            outgoing.at[s * 2 + xh],
            arr.at[xpar, y, z, xhalf],
            a_send.at[s, xh],
            a_recv.at[z, xhalf],
            z=s,
            x=xd,
            y=y,
            c=xpar,
        )

    def send_out(j, carry):
        for xh in range(2):
            own, copy = exchange(j, xh)

            @pl.when(own)
            def _():
                arr[c, y, z, xhalf] = outgoing[z * 2 + xhalf]

            @pl.when(jnp.logical_not(own))
            def _():
                copy.start()

        return carry

    lax.fori_loop(0, NZ, send_out, 0)

    for copy in loads[1:4]:
        copy.wait()
    pass_a(k_ref, v_ref, g_ref, st, tot)
    dec = jnp.exp(tot[...])
    for h in range(2):
        row = jnp.broadcast_to(dec[:, h * DK : (h + 1) * DK], (8, DK))
        hi = row.astype(BF16)
        low_part = (row - hi.astype(F32)).astype(BF16)
        for n in range(4):
            xs[n, h, 0:64, :] = st[h, n * 64 : (n + 1) * 64, :].astype(BF16)
            xs[n, h, 64:72, :] = hi
            xs[n, h, 72:80, :] = low_part
    xr[x] = xs[x]

    def x1(d):
        xd = lax.rem(x + d, NX)
        return remote(xs.at[xd], xr.at[x], x1_send.at[d - 1], x1_recv.at[x], x=xd)

    def x2(d):
        xd = lax.rem(x + d, NX)
        return remote(pbuf.at[xd], inc.at[x], x2_send.at[d - 1], x2_recv.at[x], x=xd)

    def z_copy(zd):
        return remote(zs_buf, zr.at[z], z_send.at[zd], z_recv.at[z], z=zd)

    for d in range(1, NX):
        x1(d).start()

    def state_and_decay(buf, at, h):
        got = buf[at, h].astype(F32)
        return got[0:64, :], got[64:65, :] + got[72:73, :]

    def join_row():
        for d in range(1, NX):
            src = lax.rem(x + d, NX)
            await_bytes(xr.at[src], x1_recv.at[src])
        for h in range(2):
            state, decay = state_and_decay(xr, 0, h)
            for k in range(1, NX):
                s_k, d_k = state_and_decay(xr, k, h)
                state = state * d_k + s_k
                decay = decay * d_k
            row = jnp.broadcast_to(decay, (8, DK))
            hi = row.astype(BF16)
            zs_buf[h, 0:64, :] = state.astype(BF16)
            zs_buf[h, 64:72, :] = hi
            zs_buf[h, 72:80, :] = (row - hi.astype(F32)).astype(BF16)
        for zd in range(1, NZ):

            @pl.when(zd > z)
            def _(zd=zd):
                z_copy(zd).start()

    def join_planes():
        acc[...] = jnp.zeros_like(acc)
        for zsrc in range(NZ - 1):

            @pl.when(zsrc < z)
            def _(zsrc=zsrc):
                await_bytes(zr.at[zsrc], z_recv.at[zsrc])
                for h in range(2):
                    s_k, d_k = state_and_decay(zr, zsrc, h)
                    acc[h] = acc[h] * d_k + s_k

        for h in range(2):
            state = acc[h]
            for k in range(NX):
                pbuf[k, h] = state
                s_k, d_k = state_and_decay(xr, k, h)
                state = state * d_k + s_k
        inc[x] = pbuf[x]
        for d in range(1, NX):
            x2(d).start()

    def take_state():
        for d in range(1, NX):
            src = lax.rem(x + d, NX)
            await_bytes(inc.at[src], x2_recv.at[src])
        for h in range(2):
            for n in range(4):
                st[h, n * 64 : (n + 1) * 64, :] = inc[n, h]
        loads[7].wait()

    def own_copies(s):
        here = arr.at[c, y, s]
        return [
            remote(here, here, y_send.at[0, s], y_recv.at[y, s], y=up),
            remote(here, here, y_send.at[1, s], y_recv.at[y, s], y=down),
        ]

    def to_partner(ysrc, s):
        here = arr.at[c, ysrc, s]
        return remote(here, here, p_send.at[ysrc, s], p_recv.at[ysrc, s], c=1 - c)

    def onward(ysrc, s, ydst):
        here = arr.at[c, ysrc, s]
        return remote(here, here, f_send.at[s], y_recv.at[ysrc, s], y=ydst)

    def over(s):
        return remote(part.at[1 - c, :, s], r1.at[:, s], d_send.at[s], d_recv.at[s], c=1 - c)

    def relay(s, to):
        return remote(r1.at[far, s], low.at[s], l_send.at[s], l_recv.at[s], y=to)

    def direct(s, to, side):
        return remote(r1.at[to, s], upd.at[side, s], u_send.at[s], u_recv.at[side, s], y=to)

    def joined(s, to, side):
        return remote(r1.at[to, s], upd.at[side, s], t_send.at[s], u_recv.at[side, s], y=to)

    def back(j, xh):
        own, s, xd = piece(j, xh)
        return own, remote(
            fin.at[s, xh],
            ret.at[z, xhalf],
            b_send.at[s, xh],
            b_recv.at[z, xhalf],
            z=s,
            x=xd,
            y=y,
            c=xpar,
        )

    def expert(s):
        def pack(n, carry):
            at = pl.ds(pl.multiple_of(n * width, width), width)
            xb[:, at] = arr[:, :, s, :, :, at].astype(F32).reshape(128, width).astype(BF16)
            return carry

        lax.fori_loop(0, D // width, pack, 0)
        gate = jnp.dot(xb[...], gate_w[...], preferred_element_type=F32)
        above = jnp.dot(xb[...], up_w[...], preferred_element_type=F32)
        hidden = (gate / (1.0 + jnp.exp(-gate)) * above).astype(BF16)

        def out(n, carry):
            at = pl.ds(pl.multiple_of(n * width, width), width)
            got = jnp.dot(hidden, down_w[:, at], preferred_element_type=F32)
            part[:, :, s, :, :, at] = got.reshape(2, NY, 2, 8, width).astype(BF16)
            return carry

        lax.fori_loop(0, D // width, out, 0)

    def bundle(j, lag, i):
        return (i >= lag) & (i < NZ + lag)

    def step(i, carry):
        @pl.when(bundle(i, 0, i))
        def _():
            s = near(z, i)
            for xh in range(2):
                own, _, _ = piece(i, xh)

                @pl.when(jnp.logical_not(own))
                def _(xh=xh):
                    await_bytes(arr.at[c, y, s, xh], a_recv.at[s, xh])

            for copy in own_copies(s):
                copy.start()
            to_partner(y, s).start()

        @pl.when(bundle(i, 1, i))
        def _():
            j = i - 1
            s = near(z, j)
            await_bytes(arr.at[c, down, s], y_recv.at[down, s])

            @pl.when(lax.rem(j, 2) == 0)
            def _():
                onward(down, s, up).start()

            to_partner(down, s).start()
            await_bytes(arr.at[c, up, s], y_recv.at[up, s])

            @pl.when(lax.rem(j, 2) == 1)
            def _():
                onward(up, s, down).start()

            to_partner(up, s).start()

        @pl.when(bundle(i, 2, i))
        def _():
            s = near(z, i - 2)
            await_bytes(arr.at[c, far, s], y_recv.at[far, s])
            to_partner(far, s).start()

        @pl.when(bundle(i, 5, i))
        def _():
            j = i - 5
            s = near(z, j)
            even = lax.rem(j, 2) == 0
            await_bytes(low.at[s], l_recv.at[s])
            to = jnp.where(even, down, up)
            for xh in range(2):
                r1[to, s, xh] = (r1[to, s, xh].astype(F32) + low[s, xh].astype(F32)).astype(BF16)

            @pl.when(even)
            def _():
                joined(s, down, 1).start()

            @pl.when(jnp.logical_not(even))
            def _():
                joined(s, up, 0).start()

        @pl.when(bundle(i, 4, i))
        def _():
            j = i - 4
            s = near(z, j)
            even = lax.rem(j, 2) == 0
            await_bytes(r1.at[:, s], d_recv.at[s])

            def add(n, inner):
                yy = lax.rem(y + 2 + n, NY)
                for xh in range(2):
                    r1[yy, s, xh] = (r1[yy, s, xh].astype(F32) + part[c, yy, s, xh].astype(F32)).astype(BF16)
                return inner

            lax.fori_loop(0, NY, add, 0)

            @pl.when(even)
            def _():
                relay(s, down).start()
                direct(s, up, 0).start()

            @pl.when(jnp.logical_not(even))
            def _():
                relay(s, up).start()
                direct(s, down, 1).start()

        @pl.when(bundle(i, 3, i))
        def _():
            s = near(z, i - 3)

            @pl.when(i == 3)
            def _():
                for copy in loads[4:7]:
                    copy.wait()

            for ysrc in range(NY):
                await_bytes(arr.at[1 - c, ysrc, s], p_recv.at[ysrc, s])
            expert(s)
            over(s).start()

        @pl.when(bundle(i, 6, i))
        def _():
            j = i - 6
            s = near(z, j)
            for side in range(2):
                await_bytes(upd.at[side, s], u_recv.at[side, s])
            for xh in range(2):
                total = r1[y, s, xh].astype(F32) + upd[0, s, xh].astype(F32) + upd[1, s, xh].astype(F32)
                fin[s, xh] = total.astype(BF16)
                own, copy = back(j, xh)

                @pl.when(own)
                def _(xh=xh):
                    ret[s, xh] = fin[s, xh]

                @pl.when(jnp.logical_not(own))
                def _(copy=copy):
                    copy.start()

        pl.when(i == 3)(join_row)
        pl.when(i == 6)(join_planes)
        pl.when(i == 8)(take_state)

        @pl.when(i >= 8)
        def _():
            for k in range(3):
                n = (i - 8) * 3 + k

                @pl.when(n < 16)
                def _(n=n):
                    pass_b_block(n, q_ref, k_ref, v_ref, g_ref, gain_ref, st, mixed)

        return carry

    lax.fori_loop(0, LAST, step, 0)

    def finish(j, carry):
        s = near(z, j)
        for xh in range(2):
            own, sent = exchange(j, xh)
            _, copy = back(j, xh)

            @pl.when(jnp.logical_not(own))
            def _(sent=sent, copy=copy, xh=xh):
                sent.wait_send()
                copy.wait_send()
                await_bytes(ret.at[s, xh], b_recv.at[s, xh])

        for copy in own_copies(s):
            copy.wait_send()
        await_bytes(low.at[s], f_send.at[s])
        for ysrc in range(NY):
            to_partner(ysrc, s).wait_send()
        over(s).wait_send()
        for sem in (l_send, u_send, t_send):
            await_bytes(low.at[s], sem.at[s])
        return carry

    lax.fori_loop(0, NZ, finish, 0)
    for zd in range(1, NZ):

        @pl.when(zd > z)
        def _(zd=zd):
            z_copy(zd).wait_send()

    for d in range(1, NX):
        x1(d).wait_send()
        x2(d).wait_send()

    weights = w_buf[...]
    w_hi = weights.astype(BF16)
    w_low = (weights - w_hi.astype(F32)).astype(BF16)

    def weigh(n, carry):
        at = pl.ds(pl.multiple_of(n * width, width), width)
        got_rows = ret[:, :, :, at].astype(F32).reshape(128, width).astype(BF16)
        got = lax.dot_general(w_hi, got_rows, TN, preferred_element_type=F32)
        got = got + lax.dot_general(w_low, got_rows, TN, preferred_element_type=F32)
        mine[:, at] = jnp.where(c == 0, got[0:32], got[32:64])
        cs[:, at] = jnp.where(c == 0, got[32:64], got[0:32])
        return carry

    lax.fori_loop(0, D // width, weigh, 0)
    swap = remote(cs, cr, c_send, c_recv, c=1 - c)
    swap.start()
    swap.wait()
    total = mine[...] + cr[...]
    scale = lax.rsqrt(jnp.mean(total * total, axis=-1, keepdims=True) + 1e-6)
    routed[...] = (total * scale * post_ref[...]).astype(BF16)


def everything(picks, weights, pre, post, gain, rows, gate, up, down, q, k, v, g):
    dma = pltpu.SemaphoreType.DMA
    vmem = pl.BlockSpec(memory_space=pltpu.VMEM)
    hbm = pl.BlockSpec(memory_space=pl.ANY)
    scratch = [
        pltpu.VMEM((64, D), BF16),
        pltpu.VMEM(gate.shape, BF16),
        pltpu.VMEM(up.shape, BF16),
        pltpu.VMEM(down.shape, BF16),
        pltpu.VMEM(q.shape, BF16),
        pltpu.VMEM(k.shape, BF16),
        pltpu.VMEM(v.shape, BF16),
        pltpu.VMEM(g.shape, F32),
        pltpu.VMEM((16, 8, D), BF16),
        pltpu.VMEM((128, 64), F32),
        pltpu.VMEM((2, NY, NZ, 2, 8, D), BF16),
        pltpu.VMEM((128, D), BF16),
        pltpu.VMEM((2, NY, NZ, 2, 8, D), BF16),
        pltpu.VMEM((NY, NZ, 2, 8, D), BF16),
        pltpu.VMEM((NZ, 2, 8, D), BF16),
        pltpu.VMEM((2, NZ, 2, 8, D), BF16),
        pltpu.VMEM((NZ, 2, 8, D), BF16),
        pltpu.VMEM((NZ, 2, 8, D), BF16),
        pltpu.VMEM((32, D), F32),
        pltpu.VMEM((32, D), F32),
        pltpu.VMEM((32, D), F32),
        pltpu.VMEM((2, DV, DK), F32),
        pltpu.VMEM((1, 2 * DK), F32),
        pltpu.VMEM((4, 2, 80, DK), BF16),
        pltpu.VMEM((4, 2, 80, DK), BF16),
        pltpu.VMEM((2, 80, DK), BF16),
        pltpu.VMEM((NZ, 2, 80, DK), BF16),
        pltpu.VMEM((2, 64, DK), F32),
        pltpu.VMEM((4, 2, 64, DK), F32),
        pltpu.VMEM((4, 2, 64, DK), F32),
        dma((8,)), dma((NZ, 2)), dma((NZ, 2)), dma((2, NZ)), dma((NY, NZ)), dma((NZ,)), dma((NY, NZ)), dma((NY, NZ)),
        dma((3,)), dma((4,)), dma((NZ,)), dma((NZ,)), dma((3,)), dma((4,)),
        dma((NZ,)), dma((NZ,)), dma((NZ,)), dma((NZ,)), dma((NZ,)), dma((NZ,)), dma((2, NZ)),
        dma((NZ, 2)), dma((NZ, 2)), dma(()), dma(()),
    ]
    return pl.pallas_call(
        body,
        out_shape=(
            jax.ShapeDtypeStruct((1024, 2 * DV), BF16),
            jax.ShapeDtypeStruct((32, D), BF16),
        ),
        in_specs=[vmem] * 5 + [hbm] * 8,
        out_specs=[vmem, vmem],
        scratch_shapes=scratch,
        compiler_params=pltpu.CompilerParams(collective_id=0, has_side_effects=True, vmem_limit_bytes=VLIM),
        name="everything",
    )(picks, weights, pre, post, gain, rows, gate, up, down, q, k, v, g)


def on_device(
    queries,
    key_vectors,
    value_vectors,
    decay_logit,
    head_gain,
    routed_rows,
    pre_gain,
    expert_pick,
    route_weight,
    gate_weight,
    up_weight,
    down_weight,
    post_gain,
):
    return everything(
        expert_pick.T,
        route_weight.T,
        pre_gain.reshape(1, D),
        post_gain.reshape(1, D),
        head_gain.reshape(1, DV),
        routed_rows,
        gate_weight[0],
        up_weight[0],
        down_weight[0],
        queries,
        key_vectors,
        value_vectors,
        decay_logit,
    )


def solution(mesh):
    torus = Mesh(mesh.devices.reshape(NZ, NX, NY, 2), ("z", "x", "y", "c"))
    placed = (
        P(EP, TP),
        P(EP, TP),
        P(EP, TP),
        P(EP, TP),
        P(),
        P(EP, None),
        P(),
        P(EP, None),
        P(EP, None),
        P(EP, None, TP),
        P(EP, None, TP),
        P(EP, TP, None),
        P(),
    )
    return jax.shard_map(
        on_device,
        mesh=torus,
        in_specs=placed,
        out_specs=(P(EP, TP), P(EP + TP, None)),
        check_vma=False,
    )
```

```python
import jax
import jax.numpy as jnp
from jax import lax
from jax.experimental import pallas as pl
from jax.experimental.pallas import tpu as pltpu
from jax.sharding import Mesh
from jax.sharding import PartitionSpec as P

BLK, DK, DV = 64, 128, 256
NZ, NX, NY = 8, 4, 4
D = 4096
MESH = pl.DeviceIdType.MESH
EP, TP = ("z", "x"), ("y", "c")
F32, BF16 = jnp.float32, jnp.bfloat16
VLIM = 60 * 1024 * 1024
NT = (((1,), (1,)), ((), ()))
TN = (((0,), (0,)), ((), ()))


def where_am_i():
    return tuple(lax.axis_index(a) for a in ("z", "x", "y", "c"))


def near(z, j):
    off = jnp.where(j == NZ - 1, 0, jnp.where(lax.rem(j, 2) == 0, j // 2 + 1, NZ - j // 2 - 1))
    return lax.rem(z + off, NZ)


def remote(src, dst, ssem, rsem, **to):
    return pltpu.make_async_remote_copy(
        src_ref=src, dst_ref=dst, send_sem=ssem, recv_sem=rsem, device_id=to, device_id_type=MESH
    )


def await_bytes(ref, sem):
    pltpu.make_async_copy(ref, ref, sem).wait()


def greet(groups):
    barrier = pltpu.get_barrier_semaphore()
    total = 0
    for to, is_other in groups:
        if is_other is True:
            pl.semaphore_signal(barrier, inc=1, device_id=to, device_id_type=MESH)
            total = total + 1
        else:

            @pl.when(is_other)
            def _(to=to):
                pl.semaphore_signal(barrier, inc=1, device_id=to, device_id_type=MESH)

            total = total + is_other.astype(jnp.int32)
    return barrier, total


def exchange_peers(z, x, y, c):
    peers = []
    for dz in range(NZ):
        for xh in range(2):
            zd, xd = lax.rem(z + dz, NZ), 2 * xh + c
            to = {"z": zd, "x": xd, "y": y, "c": lax.rem(x, 2)}
            peers.append((to, True if dz else jnp.logical_not((xd == x) & (lax.rem(x, 2) == c))))
    return peers


def tp_peers(y, c):
    return [
        ({"y": lax.rem(y + 1, NY)}, True),
        ({"y": lax.rem(y + NY - 1, NY)}, True),
        ({"c": 1 - c}, True),
    ]


def quarter(row, y):
    parts = [row[:, k * 64 : (k + 1) * 64] for k in range(4)]
    return jnp.where(y == 0, parts[0], jnp.where(y == 1, parts[1], jnp.where(y == 2, parts[2], parts[3])))


def slot_matrices(first_pick, second_pick, c):
    shape = (128, 64)
    i = lax.broadcasted_iota(jnp.int32, shape, 0)
    r = lax.broadcasted_iota(jnp.int32, shape, 1)
    expert = 2 * (i >> 3) + c
    same_block = (r >> 5) == ((i >> 2) & 1)
    first = (first_pick == expert) & same_block
    second = (second_pick == expert) & same_block
    named = jnp.where(first | second, 1.0, 0.0).astype(BF16)
    rr = lax.broadcasted_iota(jnp.int32, (64, 64), 0)
    cc = lax.broadcasted_iota(jnp.int32, (64, 64), 1)
    earlier = jnp.where(rr < cc, 1.0, 0.0).astype(BF16)
    rank = jnp.dot(named, earlier, preferred_element_type=F32)
    fits = rank == (i & 3).astype(F32)
    return first & fits, second & fits


def rates(logit):
    rate = (jnp.minimum(logit, 0.0) - jnp.log1p(jnp.exp(-jnp.abs(logit)))) * (1.0 / 16.0)
    hi = rate.astype(BF16)
    rest = rate - hi.astype(F32)
    mid = rest.astype(BF16)
    low = (rest - mid.astype(F32)).astype(BF16)
    rr = lax.broadcasted_iota(jnp.int32, (BLK, BLK), 0)
    cc = lax.broadcasted_iota(jnp.int32, (BLK, BLK), 1)
    lower = jnp.where(cc <= rr, 1.0, 0.0).astype(BF16)
    cum = jnp.dot(lower, low, preferred_element_type=F32)
    cum = cum + jnp.dot(lower, mid, preferred_element_type=F32)
    return cum + jnp.dot(lower, hi, preferred_element_type=F32)


def pass_a(k_ref, v_ref, g_ref, st_ref, tot_ref):
    st_ref[...] = jnp.zeros_like(st_ref)
    tot_ref[...] = jnp.zeros_like(tot_ref)

    def block(n, carry):
        at = pl.ds(n * BLK, BLK)
        cum = rates(g_ref[at, :])
        end = cum[BLK - 1 : BLK, :]
        to_end = (k_ref[at, :].astype(F32) * jnp.exp(end - cum)).astype(BF16)
        decay = jnp.exp(end)
        values = v_ref[at, :]
        for h in range(2):
            update = lax.dot_general(
                values[:, h * DV : (h + 1) * DV],
                to_end[:, h * DK : (h + 1) * DK],
                TN,
                preferred_element_type=F32,
            )
            st_ref[h] = st_ref[h] * decay[:, h * DK : (h + 1) * DK] + update
        tot_ref[...] = tot_ref[...] + end
        return carry

    lax.fori_loop(0, 16, block, 0)


def pass_b_block(n, q_ref, k_ref, v_ref, g_ref, gain_ref, st_ref, out_ref):
    at = pl.ds(pl.multiple_of(n * BLK, BLK), BLK)
    cum = rates(g_ref[at, :])
    end = cum[BLK - 1 : BLK, :]
    keys = k_ref[at, :].astype(F32)
    query_decay = (q_ref[at, :].astype(F32) * jnp.exp(cum)).astype(BF16)
    key_decay = (keys * jnp.exp(-cum)).astype(BF16)
    to_end = (keys * jnp.exp(end - cum)).astype(BF16)
    decay = jnp.exp(end)
    values = v_ref[at, :]
    rr = lax.broadcasted_iota(jnp.int32, (BLK, BLK), 0)
    cc = lax.broadcasted_iota(jnp.int32, (BLK, BLK), 1)
    for h in range(2):
        ks, vs = slice(h * DK, (h + 1) * DK), slice(h * DV, (h + 1) * DV)
        scores = lax.dot_general(query_decay[:, ks], key_decay[:, ks], NT, preferred_element_type=F32)
        weights = jnp.where(cc <= rr, scores, 0.0).astype(BF16)
        state = st_ref[h]
        total = jnp.dot(weights, values[:, vs], preferred_element_type=F32) + lax.dot_general(
            query_decay[:, ks], state.astype(BF16), NT, preferred_element_type=F32
        )
        scale = lax.rsqrt(jnp.mean(total * total, axis=-1, keepdims=True) + 1e-6)
        out_ref[at, vs] = (total * scale * gain_ref[...]).astype(BF16)
        update = lax.dot_general(values[:, vs], to_end[:, ks], TN, preferred_element_type=F32)
        st_ref[h] = state * decay[:, ks] + update


LAST = NZ + 6


def body(
    picks_ref, weight_ref, pre_ref, post_ref, gain_ref,
    rows_hbm, gate_hbm, up_hbm, down_hbm, q_hbm, k_hbm, v_hbm, g_hbm,
    mixed, routed,
    rows, gate_w, up_w, down_w, q_ref, k_ref, v_ref, g_ref,
    outgoing, w_buf, arr, xb, part, r1, low, upd, fin, ret, mine, cs, cr,
    st, tot, xs, xr, zs_buf, zr, acc, pbuf, inc,
    load, a_send, a_recv, y_send, y_recv, f_send, p_send, p_recv,
    x1_send, x1_recv, z_send, z_recv, x2_send, x2_recv,
    d_send, d_recv, l_send, l_recv, t_send, u_send, u_recv, b_send, b_recv, c_send, c_recv,
):
    z, x, y, c = where_am_i()
    up, down, far = lax.rem(y + 1, NY), lax.rem(y + NY - 1, NY), lax.rem(y + 2, NY)
    xpar, xhalf = lax.rem(x, 2), x // 2
    loads = [
        pltpu.make_async_copy(src, dst, load.at[n])
        for n, (src, dst) in enumerate(
            [
                (rows_hbm.at[pl.ds(y * 64, 64)], rows),
                (k_hbm, k_ref),
                (v_hbm, v_ref),
                (g_hbm, g_ref),
                (gate_hbm, gate_w),
                (up_hbm, up_w),
                (down_hbm, down_w),
                (q_hbm, q_ref),
            ]
        )
    ]
    for copy in loads:
        copy.start()
    groups = exchange_peers(z, x, y, c) + tp_peers(y, c)
    groups += [({"x": lax.rem(x + d, NX)}, True) for d in range(1, NX)]
    groups += [({"z": lax.rem(z + d, NZ)}, True) for d in range(1, NZ)]
    barrier, signals = greet(groups)

    first, second = slot_matrices(quarter(picks_ref[0:1, :], y), quarter(picks_ref[1:2, :], y), c)
    w_buf[...] = jnp.where(first, quarter(weight_ref[0:1, :], y), 0.0) + jnp.where(
        second, quarter(weight_ref[1:2, :], y), 0.0
    )
    select = jnp.where(first | second, 1.0, 0.0).astype(BF16)
    loads[0].wait()
    wide = rows[...].astype(F32)
    scale = lax.rsqrt(jnp.mean(wide * wide, axis=-1, keepdims=True) + 1e-6)
    width = 512
    for n in range(0, D, width):
        normed = (wide[:, n : n + width] * scale * pre_ref[:, n : n + width]).astype(BF16)
        got = jnp.dot(select, normed, preferred_element_type=F32)
        outgoing[:, :, n : n + width] = got.reshape(16, 8, width).astype(BF16)
    pl.semaphore_wait(barrier, signals)

    def piece(j, xh):
        s, xd = near(z, j), 2 * xh + c
        return (s == z) & (xd == x) & (xpar == c), s, xd

    def exchange(j, xh):
        own, s, xd = piece(j, xh)
        return own, remote(
            outgoing.at[s * 2 + xh],
            arr.at[xpar, y, z, xhalf],
            a_send.at[s, xh],
            a_recv.at[z, xhalf],
            z=s,
            x=xd,
            y=y,
            c=xpar,
        )

    def send_out(j, carry):
        for xh in range(2):
            own, copy = exchange(j, xh)

            @pl.when(own)
            def _():
                arr[c, y, z, xhalf] = outgoing[z * 2 + xhalf]

            @pl.when(jnp.logical_not(own))
            def _():
                copy.start()

        return carry

    lax.fori_loop(0, NZ, send_out, 0)

    for copy in loads[1:4]:
        copy.wait()
    pass_a(k_ref, v_ref, g_ref, st, tot)
    dec = jnp.exp(tot[...])
    for h in range(2):
        row = jnp.broadcast_to(dec[:, h * DK : (h + 1) * DK], (8, DK))
        hi = row.astype(BF16)
        low_part = (row - hi.astype(F32)).astype(BF16)
        for n in range(4):
            xs[n, h, 0:64, :] = st[h, n * 64 : (n + 1) * 64, :].astype(BF16)
            xs[n, h, 64:72, :] = hi
            xs[n, h, 72:80, :] = low_part
    xr[x] = xs[x]

    def x1(d):
        xd = lax.rem(x + d, NX)
        return remote(xs.at[xd], xr.at[x], x1_send.at[d - 1], x1_recv.at[x], x=xd)

    def x2(d):
        xd = lax.rem(x + d, NX)
        return remote(pbuf.at[xd], inc.at[x], x2_send.at[d - 1], x2_recv.at[x], x=xd)

    def z_copy(zd):
        return remote(zs_buf, zr.at[z], z_send.at[zd], z_recv.at[z], z=zd)

    for d in range(1, NX):
        x1(d).start()

    def state_and_decay(buf, at, h):
        got = buf[at, h].astype(F32)
        return got[0:64, :], got[64:65, :] + got[72:73, :]

    def join_row():
        for d in range(1, NX):
            src = lax.rem(x + d, NX)
            await_bytes(xr.at[src], x1_recv.at[src])
        for h in range(2):
            state, decay = state_and_decay(xr, 0, h)
            for k in range(1, NX):
                s_k, d_k = state_and_decay(xr, k, h)
                state = state * d_k + s_k
                decay = decay * d_k
            row = jnp.broadcast_to(decay, (8, DK))
            hi = row.astype(BF16)
            zs_buf[h, 0:64, :] = state.astype(BF16)
            zs_buf[h, 64:72, :] = hi
            zs_buf[h, 72:80, :] = (row - hi.astype(F32)).astype(BF16)
        for zd in range(1, NZ):

            @pl.when(zd > z)
            def _(zd=zd):
                z_copy(zd).start()

    def join_planes():
        acc[...] = jnp.zeros_like(acc)
        for zsrc in range(NZ - 1):

            @pl.when(zsrc < z)
            def _(zsrc=zsrc):
                await_bytes(zr.at[zsrc], z_recv.at[zsrc])
                for h in range(2):
                    s_k, d_k = state_and_decay(zr, zsrc, h)
                    acc[h] = acc[h] * d_k + s_k

        for h in range(2):
            state = acc[h]
            for k in range(NX):
                pbuf[k, h] = state
                s_k, d_k = state_and_decay(xr, k, h)
                state = state * d_k + s_k
        inc[x] = pbuf[x]
        for d in range(1, NX):
            x2(d).start()

    def take_state():
        for d in range(1, NX):
            src = lax.rem(x + d, NX)
            await_bytes(inc.at[src], x2_recv.at[src])
        for h in range(2):
            for n in range(4):
                st[h, n * 64 : (n + 1) * 64, :] = inc[n, h]
        loads[7].wait()

    def own_copies(s):
        here = arr.at[c, y, s]
        return [
            remote(here, here, y_send.at[0, s], y_recv.at[y, s], y=up),
            remote(here, here, y_send.at[1, s], y_recv.at[y, s], y=down),
        ]

    def to_partner(ysrc, s):
        here = arr.at[c, ysrc, s]
        return remote(here, here, p_send.at[ysrc, s], p_recv.at[ysrc, s], c=1 - c)

    def onward(ysrc, s, ydst):
        here = arr.at[c, ysrc, s]
        return remote(here, here, f_send.at[s], y_recv.at[ysrc, s], y=ydst)

    def over(s):
        return remote(part.at[1 - c, :, s], r1.at[:, s], d_send.at[s], d_recv.at[s], c=1 - c)

    def relay(s, to):
        return remote(r1.at[far, s], low.at[s], l_send.at[s], l_recv.at[s], y=to)

    def direct(s, to, side):
        return remote(r1.at[to, s], upd.at[side, s], u_send.at[s], u_recv.at[side, s], y=to)

    def joined(s, to, side):
        return remote(r1.at[to, s], upd.at[side, s], t_send.at[s], u_recv.at[side, s], y=to)

    def back(j, xh):
        own, s, xd = piece(j, xh)
        return own, remote(
            fin.at[s, xh],
            ret.at[z, xhalf],
            b_send.at[s, xh],
            b_recv.at[z, xhalf],
            z=s,
            x=xd,
            y=y,
            c=xpar,
        )

    def expert(s):
        def pack(n, carry):
            at = pl.ds(pl.multiple_of(n * width, width), width)
            xb[:, at] = arr[:, :, s, :, :, at].astype(F32).reshape(128, width).astype(BF16)
            return carry

        lax.fori_loop(0, D // width, pack, 0)
        gate = jnp.dot(xb[...], gate_w[...], preferred_element_type=F32)
        above = jnp.dot(xb[...], up_w[...], preferred_element_type=F32)
        hidden = (gate / (1.0 + jnp.exp(-gate)) * above).astype(BF16)

        def out(n, carry):
            at = pl.ds(pl.multiple_of(n * width, width), width)
            got = jnp.dot(hidden, down_w[:, at], preferred_element_type=F32)
            part[:, :, s, :, :, at] = got.reshape(2, NY, 2, 8, width).astype(BF16)
            return carry

        lax.fori_loop(0, D // width, out, 0)

    def bundle(j, lag, i):
        return (i >= lag) & (i < NZ + lag)

    def step(i, carry):
        @pl.when(bundle(i, 0, i))
        def _():
            s = near(z, i)
            for xh in range(2):
                own, _, _ = piece(i, xh)

                @pl.when(jnp.logical_not(own))
                def _(xh=xh):
                    await_bytes(arr.at[c, y, s, xh], a_recv.at[s, xh])

            for copy in own_copies(s):
                copy.start()
            to_partner(y, s).start()

        @pl.when(bundle(i, 1, i))
        def _():
            j = i - 1
            s = near(z, j)
            await_bytes(arr.at[c, down, s], y_recv.at[down, s])

            @pl.when(lax.rem(j, 2) == 0)
            def _():
                onward(down, s, up).start()

            to_partner(down, s).start()
            await_bytes(arr.at[c, up, s], y_recv.at[up, s])

            @pl.when(lax.rem(j, 2) == 1)
            def _():
                onward(up, s, down).start()

            to_partner(up, s).start()

        @pl.when(bundle(i, 2, i))
        def _():
            s = near(z, i - 2)
            await_bytes(arr.at[c, far, s], y_recv.at[far, s])
            to_partner(far, s).start()

        @pl.when(bundle(i, 5, i))
        def _():
            j = i - 5
            s = near(z, j)
            even = lax.rem(j, 2) == 0
            await_bytes(low.at[s], l_recv.at[s])
            to = jnp.where(even, down, up)
            for xh in range(2):
                r1[to, s, xh] = (r1[to, s, xh].astype(F32) + low[s, xh].astype(F32)).astype(BF16)

            @pl.when(even)
            def _():
                joined(s, down, 1).start()

            @pl.when(jnp.logical_not(even))
            def _():
                joined(s, up, 0).start()

        @pl.when(bundle(i, 4, i))
        def _():
            j = i - 4
            s = near(z, j)
            even = lax.rem(j, 2) == 0
            await_bytes(r1.at[:, s], d_recv.at[s])

            def add(n, inner):
                yy = lax.rem(y + 2 + n, NY)
                for xh in range(2):
                    r1[yy, s, xh] = (r1[yy, s, xh].astype(F32) + part[c, yy, s, xh].astype(F32)).astype(BF16)
                return inner

            lax.fori_loop(0, NY, add, 0)

            @pl.when(even)
            def _():
                relay(s, down).start()
                direct(s, up, 0).start()

            @pl.when(jnp.logical_not(even))
            def _():
                relay(s, up).start()
                direct(s, down, 1).start()

        @pl.when(bundle(i, 3, i))
        def _():
            s = near(z, i - 3)

            @pl.when(i == 3)
            def _():
                for copy in loads[4:7]:
                    copy.wait()

            for ysrc in range(NY):
                await_bytes(arr.at[1 - c, ysrc, s], p_recv.at[ysrc, s])
            expert(s)
            over(s).start()

        @pl.when(bundle(i, 6, i))
        def _():
            j = i - 6
            s = near(z, j)
            for side in range(2):
                await_bytes(upd.at[side, s], u_recv.at[side, s])
            for xh in range(2):
                total = r1[y, s, xh].astype(F32) + upd[0, s, xh].astype(F32) + upd[1, s, xh].astype(F32)
                fin[s, xh] = total.astype(BF16)
                own, copy = back(j, xh)

                @pl.when(own)
                def _(xh=xh):
                    ret[s, xh] = fin[s, xh]

                @pl.when(jnp.logical_not(own))
                def _(copy=copy):
                    copy.start()

        pl.when(i == 3)(join_row)
        pl.when(i == 6)(join_planes)
        pl.when(i == 8)(take_state)

        @pl.when(i >= 8)
        def _():
            for k in range(3):
                n = (i - 8) * 3 + k

                @pl.when(n < 16)
                def _(n=n):
                    pass_b_block(n, q_ref, k_ref, v_ref, g_ref, gain_ref, st, mixed)

        return carry

    lax.fori_loop(0, LAST, step, 0)

    def finish(j, carry):
        s = near(z, j)
        for xh in range(2):
            own, sent = exchange(j, xh)
            _, copy = back(j, xh)

            @pl.when(jnp.logical_not(own))
            def _(sent=sent, copy=copy, xh=xh):
                sent.wait_send()
                copy.wait_send()
                await_bytes(ret.at[s, xh], b_recv.at[s, xh])

        for copy in own_copies(s):
            copy.wait_send()
        await_bytes(low.at[s], f_send.at[s])
        for ysrc in range(NY):
            to_partner(ysrc, s).wait_send()
        over(s).wait_send()
        for sem in (l_send, u_send, t_send):
            await_bytes(low.at[s], sem.at[s])
        return carry

    lax.fori_loop(0, NZ, finish, 0)
    for zd in range(1, NZ):

        @pl.when(zd > z)
        def _(zd=zd):
            z_copy(zd).wait_send()

    for d in range(1, NX):
        x1(d).wait_send()
        x2(d).wait_send()

    weights = w_buf[...]
    w_hi = weights.astype(BF16)
    w_low = (weights - w_hi.astype(F32)).astype(BF16)

    def weigh(n, carry):
        at = pl.ds(pl.multiple_of(n * width, width), width)
        got_rows = ret[:, :, :, at].astype(F32).reshape(128, width).astype(BF16)
        got = lax.dot_general(w_hi, got_rows, TN, preferred_element_type=F32)
        got = got + lax.dot_general(w_low, got_rows, TN, preferred_element_type=F32)
        mine[:, at] = jnp.where(c == 0, got[0:32], got[32:64])
        cs[n] = jnp.where(c == 0, got[32:64], got[0:32])
        swap(n).start()
        return carry

    def swap(n):
        return remote(cs.at[n], cr.at[n], c_send.at[n], c_recv.at[n], c=1 - c)

    def join(n, carry):
        at = pl.ds(pl.multiple_of(n * width, width), width)
        swap(n).wait()
        mine[:, at] = mine[:, at] + cr[n]
        return carry

    lax.fori_loop(0, D // width, weigh, 0)
    lax.fori_loop(0, D // width, join, 0)
    total = mine[...]
    scale = lax.rsqrt(jnp.mean(total * total, axis=-1, keepdims=True) + 1e-6)
    routed[...] = (total * scale * post_ref[...]).astype(BF16)


def everything(picks, weights, pre, post, gain, rows, gate, up, down, q, k, v, g):
    dma = pltpu.SemaphoreType.DMA
    vmem = pl.BlockSpec(memory_space=pltpu.VMEM)
    hbm = pl.BlockSpec(memory_space=pl.ANY)
    scratch = [
        pltpu.VMEM((64, D), BF16),
        pltpu.VMEM(gate.shape, BF16),
        pltpu.VMEM(up.shape, BF16),
        pltpu.VMEM(down.shape, BF16),
        pltpu.VMEM(q.shape, BF16),
        pltpu.VMEM(k.shape, BF16),
        pltpu.VMEM(v.shape, BF16),
        pltpu.VMEM(g.shape, F32),
        pltpu.VMEM((16, 8, D), BF16),
        pltpu.VMEM((128, 64), F32),
        pltpu.VMEM((2, NY, NZ, 2, 8, D), BF16),
        pltpu.VMEM((128, D), BF16),
        pltpu.VMEM((2, NY, NZ, 2, 8, D), BF16),
        pltpu.VMEM((NY, NZ, 2, 8, D), BF16),
        pltpu.VMEM((NZ, 2, 8, D), BF16),
        pltpu.VMEM((2, NZ, 2, 8, D), BF16),
        pltpu.VMEM((NZ, 2, 8, D), BF16),
        pltpu.VMEM((NZ, 2, 8, D), BF16),
        pltpu.VMEM((32, D), F32),
        pltpu.VMEM((8, 32, D // 8), F32),
        pltpu.VMEM((8, 32, D // 8), F32),
        pltpu.VMEM((2, DV, DK), F32),
        pltpu.VMEM((1, 2 * DK), F32),
        pltpu.VMEM((4, 2, 80, DK), BF16),
        pltpu.VMEM((4, 2, 80, DK), BF16),
        pltpu.VMEM((2, 80, DK), BF16),
        pltpu.VMEM((NZ, 2, 80, DK), BF16),
        pltpu.VMEM((2, 64, DK), F32),
        pltpu.VMEM((4, 2, 64, DK), F32),
        pltpu.VMEM((4, 2, 64, DK), F32),
        dma((8,)), dma((NZ, 2)), dma((NZ, 2)), dma((2, NZ)), dma((NY, NZ)), dma((NZ,)), dma((NY, NZ)), dma((NY, NZ)),
        dma((3,)), dma((4,)), dma((NZ,)), dma((NZ,)), dma((3,)), dma((4,)),
        dma((NZ,)), dma((NZ,)), dma((NZ,)), dma((NZ,)), dma((NZ,)), dma((NZ,)), dma((2, NZ)),
        dma((NZ, 2)), dma((NZ, 2)), dma((8,)), dma((8,)),
    ]
    return pl.pallas_call(
        body,
        out_shape=(
            jax.ShapeDtypeStruct((1024, 2 * DV), BF16),
            jax.ShapeDtypeStruct((32, D), BF16),
        ),
        in_specs=[vmem] * 5 + [hbm] * 8,
        out_specs=[vmem, vmem],
        scratch_shapes=scratch,
        compiler_params=pltpu.CompilerParams(collective_id=0, has_side_effects=True, vmem_limit_bytes=VLIM),
        name="everything",
    )(picks, weights, pre, post, gain, rows, gate, up, down, q, k, v, g)


def on_device(
    queries,
    key_vectors,
    value_vectors,
    decay_logit,
    head_gain,
    routed_rows,
    pre_gain,
    expert_pick,
    route_weight,
    gate_weight,
    up_weight,
    down_weight,
    post_gain,
):
    return everything(
        expert_pick.T,
        route_weight.T,
        pre_gain.reshape(1, D),
        post_gain.reshape(1, D),
        head_gain.reshape(1, DV),
        routed_rows,
        gate_weight[0],
        up_weight[0],
        down_weight[0],
        queries,
        key_vectors,
        value_vectors,
        decay_logit,
    )


def solution(mesh):
    torus = Mesh(mesh.devices.reshape(NZ, NX, NY, 2), ("z", "x", "y", "c"))
    placed = (
        P(EP, TP),
        P(EP, TP),
        P(EP, TP),
        P(EP, TP),
        P(),
        P(EP, None),
        P(),
        P(EP, None),
        P(EP, None),
        P(EP, None, TP),
        P(EP, None, TP),
        P(EP, TP, None),
        P(),
    )
    return jax.shard_map(
        on_device,
        mesh=torus,
        in_specs=placed,
        out_specs=(P(EP, TP), P(EP + TP, None)),
        check_vma=False,
    )
```

```python
import jax
import jax.numpy as jnp
from jax import lax
from jax.experimental import pallas as pl
from jax.experimental.pallas import tpu as pltpu
from jax.sharding import Mesh
from jax.sharding import PartitionSpec as P

BLK, DK, DV = 64, 128, 256
NZ, NX, NY = 8, 4, 4
D = 4096
MESH = pl.DeviceIdType.MESH
EP, TP = ("z", "x"), ("y", "c")
F32, BF16 = jnp.float32, jnp.bfloat16
VLIM = 60 * 1024 * 1024
NT = (((1,), (1,)), ((), ()))
TN = (((0,), (0,)), ((), ()))


def where_am_i():
    return tuple(lax.axis_index(a) for a in ("z", "x", "y", "c"))


def near(z, j):
    off = jnp.where(j == NZ - 1, 0, jnp.where(lax.rem(j, 2) == 0, j // 2 + 1, NZ - j // 2 - 1))
    return lax.rem(z + off, NZ)


def remote(src, dst, ssem, rsem, **to):
    return pltpu.make_async_remote_copy(
        src_ref=src, dst_ref=dst, send_sem=ssem, recv_sem=rsem, device_id=to, device_id_type=MESH
    )


def await_bytes(ref, sem):
    pltpu.make_async_copy(ref, ref, sem).wait()


def greet(groups):
    barrier = pltpu.get_barrier_semaphore()
    total = 0
    for to, is_other in groups:
        if is_other is True:
            pl.semaphore_signal(barrier, inc=1, device_id=to, device_id_type=MESH)
            total = total + 1
        else:

            @pl.when(is_other)
            def _(to=to):
                pl.semaphore_signal(barrier, inc=1, device_id=to, device_id_type=MESH)

            total = total + is_other.astype(jnp.int32)
    return barrier, total


def exchange_peers(z, x, y, c):
    peers = []
    for dz in range(NZ):
        for xh in range(2):
            zd, xd = lax.rem(z + dz, NZ), 2 * xh + c
            to = {"z": zd, "x": xd, "y": y, "c": lax.rem(x, 2)}
            peers.append((to, True if dz else jnp.logical_not((xd == x) & (lax.rem(x, 2) == c))))
    return peers


def tp_peers(y, c):
    return [
        ({"y": lax.rem(y + 1, NY)}, True),
        ({"y": lax.rem(y + NY - 1, NY)}, True),
        ({"c": 1 - c}, True),
    ]


def quarter(row, y):
    parts = [row[:, k * 64 : (k + 1) * 64] for k in range(4)]
    return jnp.where(y == 0, parts[0], jnp.where(y == 1, parts[1], jnp.where(y == 2, parts[2], parts[3])))


def slot_matrices(first_pick, second_pick, c):
    shape = (128, 64)
    i = lax.broadcasted_iota(jnp.int32, shape, 0)
    r = lax.broadcasted_iota(jnp.int32, shape, 1)
    expert = 2 * (i >> 3) + c
    same_block = (r >> 5) == ((i >> 2) & 1)
    first = (first_pick == expert) & same_block
    second = (second_pick == expert) & same_block
    named = jnp.where(first | second, 1.0, 0.0).astype(BF16)
    rr = lax.broadcasted_iota(jnp.int32, (64, 64), 0)
    cc = lax.broadcasted_iota(jnp.int32, (64, 64), 1)
    earlier = jnp.where(rr < cc, 1.0, 0.0).astype(BF16)
    rank = jnp.dot(named, earlier, preferred_element_type=F32)
    fits = rank == (i & 3).astype(F32)
    return first & fits, second & fits


def rates(logit):
    rate = (jnp.minimum(logit, 0.0) - jnp.log1p(jnp.exp(-jnp.abs(logit)))) * (1.0 / 16.0)
    hi = rate.astype(BF16)
    rest = rate - hi.astype(F32)
    mid = rest.astype(BF16)
    low = (rest - mid.astype(F32)).astype(BF16)
    rr = lax.broadcasted_iota(jnp.int32, (BLK, BLK), 0)
    cc = lax.broadcasted_iota(jnp.int32, (BLK, BLK), 1)
    lower = jnp.where(cc <= rr, 1.0, 0.0).astype(BF16)
    cum = jnp.dot(lower, low, preferred_element_type=F32)
    cum = cum + jnp.dot(lower, mid, preferred_element_type=F32)
    return cum + jnp.dot(lower, hi, preferred_element_type=F32)


def pass_a(k_ref, v_ref, g_ref, st_ref, tot_ref):
    st_ref[...] = jnp.zeros_like(st_ref)
    tot_ref[...] = jnp.zeros_like(tot_ref)

    def block(n, carry):
        at = pl.ds(n * BLK, BLK)
        cum = rates(g_ref[at, :])
        end = cum[BLK - 1 : BLK, :]
        to_end = (k_ref[at, :].astype(F32) * jnp.exp(end - cum)).astype(BF16)
        decay = jnp.exp(end)
        values = v_ref[at, :]
        for h in range(2):
            update = lax.dot_general(
                values[:, h * DV : (h + 1) * DV],
                to_end[:, h * DK : (h + 1) * DK],
                TN,
                preferred_element_type=F32,
            )
            st_ref[h] = st_ref[h] * decay[:, h * DK : (h + 1) * DK] + update
        tot_ref[...] = tot_ref[...] + end
        return carry

    lax.fori_loop(0, 16, block, 0)


def pass_b_block(n, q_ref, k_ref, v_ref, g_ref, gain_ref, st_ref, out_ref):
    at = pl.ds(pl.multiple_of(n * BLK, BLK), BLK)
    cum = rates(g_ref[at, :])
    end = cum[BLK - 1 : BLK, :]
    keys = k_ref[at, :].astype(F32)
    query_decay = (q_ref[at, :].astype(F32) * jnp.exp(cum)).astype(BF16)
    key_decay = (keys * jnp.exp(-cum)).astype(BF16)
    to_end = (keys * jnp.exp(end - cum)).astype(BF16)
    decay = jnp.exp(end)
    values = v_ref[at, :]
    rr = lax.broadcasted_iota(jnp.int32, (BLK, BLK), 0)
    cc = lax.broadcasted_iota(jnp.int32, (BLK, BLK), 1)
    for h in range(2):
        ks, vs = slice(h * DK, (h + 1) * DK), slice(h * DV, (h + 1) * DV)
        scores = lax.dot_general(query_decay[:, ks], key_decay[:, ks], NT, preferred_element_type=F32)
        weights = jnp.where(cc <= rr, scores, 0.0).astype(BF16)
        state = st_ref[h]
        total = jnp.dot(weights, values[:, vs], preferred_element_type=F32) + lax.dot_general(
            query_decay[:, ks], state.astype(BF16), NT, preferred_element_type=F32
        )
        scale = lax.rsqrt(jnp.mean(total * total, axis=-1, keepdims=True) + 1e-6)
        out_ref[at, vs] = (total * scale * gain_ref[...]).astype(BF16)
        update = lax.dot_general(values[:, vs], to_end[:, ks], TN, preferred_element_type=F32)
        st_ref[h] = state * decay[:, ks] + update


LAST = NZ + 5


def body(
    picks_ref, weight_ref, pre_ref, post_ref, gain_ref,
    rows_hbm, gate_hbm, up_hbm, down_hbm, q_hbm, k_hbm, v_hbm, g_hbm,
    mixed, routed,
    rows, gate_w, up_w, down_w, q_ref, k_ref, v_ref, g_ref,
    outgoing, w_buf, arr, xb, part, r1, low, upd, fin, ret, mine, cs, cr,
    st, tot, xs, xr, zs_buf, zr, acc, pbuf, inc,
    load, a_send, a_recv, y_send, y_recv, f_send, p_send, p_recv,
    x1_send, x1_recv, z_send, z_recv, x2_send, x2_recv,
    d_send, d_recv, l_send, l_recv, t_send, u_send, u_recv, b_send, b_recv, c_send, c_recv,
):
    z, x, y, c = where_am_i()
    up, down, far = lax.rem(y + 1, NY), lax.rem(y + NY - 1, NY), lax.rem(y + 2, NY)
    xpar, xhalf = lax.rem(x, 2), x // 2
    loads = [
        pltpu.make_async_copy(src, dst, load.at[n])
        for n, (src, dst) in enumerate(
            [
                (rows_hbm.at[pl.ds(y * 64, 64)], rows),
                (k_hbm, k_ref),
                (v_hbm, v_ref),
                (g_hbm, g_ref),
                (gate_hbm, gate_w),
                (up_hbm, up_w),
                (down_hbm, down_w),
                (q_hbm, q_ref),
            ]
        )
    ]
    for copy in loads:
        copy.start()
    groups = exchange_peers(z, x, y, c) + tp_peers(y, c)
    groups += [({"x": lax.rem(x + d, NX)}, True) for d in range(1, NX)]
    groups += [({"z": lax.rem(z + d, NZ)}, True) for d in range(1, NZ)]
    barrier, signals = greet(groups)

    first, second = slot_matrices(quarter(picks_ref[0:1, :], y), quarter(picks_ref[1:2, :], y), c)
    w_buf[...] = jnp.where(first, quarter(weight_ref[0:1, :], y), 0.0) + jnp.where(
        second, quarter(weight_ref[1:2, :], y), 0.0
    )
    select = jnp.where(first | second, 1.0, 0.0).astype(BF16)
    loads[0].wait()
    wide = rows[...].astype(F32)
    scale = lax.rsqrt(jnp.mean(wide * wide, axis=-1, keepdims=True) + 1e-6)
    width = 512
    for n in range(0, D, width):
        normed = (wide[:, n : n + width] * scale * pre_ref[:, n : n + width]).astype(BF16)
        got = jnp.dot(select, normed, preferred_element_type=F32)
        outgoing[:, :, n : n + width] = got.reshape(16, 8, width).astype(BF16)
    pl.semaphore_wait(barrier, signals)

    def piece(j, xh):
        s, xd = near(z, j), 2 * xh + c
        return (s == z) & (xd == x) & (xpar == c), s, xd

    def exchange(j, xh):
        own, s, xd = piece(j, xh)
        return own, remote(
            outgoing.at[s * 2 + xh],
            arr.at[xpar, y, z, xhalf],
            a_send.at[s, xh],
            a_recv.at[z, xhalf],
            z=s,
            x=xd,
            y=y,
            c=xpar,
        )

    def send_out(j, carry):
        for xh in range(2):
            own, copy = exchange(j, xh)

            @pl.when(own)
            def _():
                arr[c, y, z, xhalf] = outgoing[z * 2 + xhalf]

            @pl.when(jnp.logical_not(own))
            def _():
                copy.start()

        return carry

    lax.fori_loop(0, NZ, send_out, 0)

    for copy in loads[1:4]:
        copy.wait()
    pass_a(k_ref, v_ref, g_ref, st, tot)
    dec = jnp.exp(tot[...])
    for h in range(2):
        row = jnp.broadcast_to(dec[:, h * DK : (h + 1) * DK], (8, DK))
        hi = row.astype(BF16)
        low_part = (row - hi.astype(F32)).astype(BF16)
        for n in range(4):
            xs[n, h, 0:64, :] = st[h, n * 64 : (n + 1) * 64, :].astype(BF16)
            xs[n, h, 64:72, :] = hi
            xs[n, h, 72:80, :] = low_part
    xr[x] = xs[x]

    def x1(d):
        xd = lax.rem(x + d, NX)
        return remote(xs.at[xd], xr.at[x], x1_send.at[d - 1], x1_recv.at[x], x=xd)

    def x2(d):
        xd = lax.rem(x + d, NX)
        return remote(pbuf.at[xd], inc.at[x], x2_send.at[d - 1], x2_recv.at[x], x=xd)

    def z_copy(zd):
        return remote(zs_buf, zr.at[z], z_send.at[zd], z_recv.at[z], z=zd)

    for d in range(1, NX):
        x1(d).start()

    def state_and_decay(buf, at, h):
        got = buf[at, h].astype(F32)
        return got[0:64, :], got[64:65, :] + got[72:73, :]

    def join_row():
        for d in range(1, NX):
            src = lax.rem(x + d, NX)
            await_bytes(xr.at[src], x1_recv.at[src])
        for h in range(2):
            state, decay = state_and_decay(xr, 0, h)
            for k in range(1, NX):
                s_k, d_k = state_and_decay(xr, k, h)
                state = state * d_k + s_k
                decay = decay * d_k
            row = jnp.broadcast_to(decay, (8, DK))
            hi = row.astype(BF16)
            zs_buf[h, 0:64, :] = state.astype(BF16)
            zs_buf[h, 64:72, :] = hi
            zs_buf[h, 72:80, :] = (row - hi.astype(F32)).astype(BF16)
        for zd in range(1, NZ):

            @pl.when(zd > z)
            def _(zd=zd):
                z_copy(zd).start()

    def join_planes():
        acc[...] = jnp.zeros_like(acc)
        for zsrc in range(NZ - 1):

            @pl.when(zsrc < z)
            def _(zsrc=zsrc):
                await_bytes(zr.at[zsrc], z_recv.at[zsrc])
                for h in range(2):
                    s_k, d_k = state_and_decay(zr, zsrc, h)
                    acc[h] = acc[h] * d_k + s_k

        for h in range(2):
            state = acc[h]
            for k in range(NX):
                pbuf[k, h] = state
                s_k, d_k = state_and_decay(xr, k, h)
                state = state * d_k + s_k
        inc[x] = pbuf[x]
        for d in range(1, NX):
            x2(d).start()

    def take_state():
        for d in range(1, NX):
            src = lax.rem(x + d, NX)
            await_bytes(inc.at[src], x2_recv.at[src])
        for h in range(2):
            for n in range(4):
                st[h, n * 64 : (n + 1) * 64, :] = inc[n, h]
        loads[7].wait()

    def own_copies(s):
        here = arr.at[c, y, s]
        return [
            remote(here, here, y_send.at[0, s], y_recv.at[y, s], y=up),
            remote(here, here, y_send.at[1, s], y_recv.at[y, s], y=down),
        ]

    def to_partner(ysrc, s):
        here = arr.at[c, ysrc, s]
        return remote(here, here, p_send.at[ysrc, s], p_recv.at[ysrc, s], c=1 - c)

    def onward(ysrc, s, ydst):
        here = arr.at[c, ysrc, s]
        return remote(here, here, f_send.at[s], y_recv.at[ysrc, s], y=ydst)

    def over(s):
        return remote(part.at[1 - c, :, s], r1.at[:, s], d_send.at[s], d_recv.at[s], c=1 - c)

    def relay(s, to):
        return remote(r1.at[far, s], low.at[s], l_send.at[s], l_recv.at[s], y=to)

    def direct(s, to, side):
        return remote(r1.at[to, s], upd.at[side, s], u_send.at[s], u_recv.at[side, s], y=to)

    def joined(s, to, side):
        return remote(r1.at[to, s], upd.at[side, s], t_send.at[s], u_recv.at[side, s], y=to)

    def back(j, xh):
        own, s, xd = piece(j, xh)
        return own, remote(
            fin.at[s, xh],
            ret.at[z, xhalf],
            b_send.at[s, xh],
            b_recv.at[z, xhalf],
            z=s,
            x=xd,
            y=y,
            c=xpar,
        )

    def expert(s):
        def pack(n, carry):
            at = pl.ds(pl.multiple_of(n * width, width), width)
            xb[:, at] = arr[:, :, s, :, :, at].astype(F32).reshape(128, width).astype(BF16)
            return carry

        lax.fori_loop(0, D // width, pack, 0)
        gate = jnp.dot(xb[...], gate_w[...], preferred_element_type=F32)
        above = jnp.dot(xb[...], up_w[...], preferred_element_type=F32)
        hidden = (gate / (1.0 + jnp.exp(-gate)) * above).astype(BF16)

        def out(n, carry):
            at = pl.ds(pl.multiple_of(n * width, width), width)
            got = jnp.dot(hidden, down_w[:, at], preferred_element_type=F32)
            part[:, :, s, :, :, at] = got.reshape(2, NY, 2, 8, width).astype(BF16)
            return carry

        lax.fori_loop(0, D // width, out, 0)

    def bundle(j, lag, i):
        return (i >= lag) & (i < NZ + lag)

    def step(i, carry):
        @pl.when(bundle(i, 0, i))
        def _():
            s = near(z, i)
            for xh in range(2):
                own, _, _ = piece(i, xh)

                @pl.when(jnp.logical_not(own))
                def _(xh=xh):
                    await_bytes(arr.at[c, y, s, xh], a_recv.at[s, xh])

            for copy in own_copies(s):
                copy.start()
            to_partner(y, s).start()

        @pl.when(bundle(i, 1, i))
        def _():
            j = i - 1
            s = near(z, j)
            await_bytes(arr.at[c, down, s], y_recv.at[down, s])

            @pl.when(lax.rem(j, 2) == 0)
            def _():
                onward(down, s, up).start()

            to_partner(down, s).start()
            await_bytes(arr.at[c, up, s], y_recv.at[up, s])

            @pl.when(lax.rem(j, 2) == 1)
            def _():
                onward(up, s, down).start()

            to_partner(up, s).start()

        @pl.when(bundle(i, 2, i))
        def _():
            s = near(z, i - 2)
            await_bytes(arr.at[c, far, s], y_recv.at[far, s])
            to_partner(far, s).start()

        @pl.when(bundle(i, 4, i))
        def _():
            j = i - 4
            s = near(z, j)
            even = lax.rem(j, 2) == 0
            await_bytes(low.at[s], l_recv.at[s])
            to = jnp.where(even, down, up)
            for xh in range(2):
                r1[to, s, xh] = (r1[to, s, xh].astype(F32) + low[s, xh].astype(F32)).astype(BF16)

            @pl.when(even)
            def _():
                joined(s, down, 1).start()

            @pl.when(jnp.logical_not(even))
            def _():
                joined(s, up, 0).start()

        @pl.when(bundle(i, 3, i))
        def _():
            j = i - 3
            s = near(z, j)
            even = lax.rem(j, 2) == 0
            await_bytes(r1.at[:, s], d_recv.at[s])

            def add(n, inner):
                yy = lax.rem(y + 2 + n, NY)
                for xh in range(2):
                    r1[yy, s, xh] = (r1[yy, s, xh].astype(F32) + part[c, yy, s, xh].astype(F32)).astype(BF16)
                return inner

            lax.fori_loop(0, NY, add, 0)

            @pl.when(even)
            def _():
                relay(s, down).start()
                direct(s, up, 0).start()

            @pl.when(jnp.logical_not(even))
            def _():
                relay(s, up).start()
                direct(s, down, 1).start()

        @pl.when(bundle(i, 2, i))
        def _():
            s = near(z, i - 2)

            @pl.when(i == 2)
            def _():
                for copy in loads[4:7]:
                    copy.wait()

            for ysrc in range(NY):
                await_bytes(arr.at[1 - c, ysrc, s], p_recv.at[ysrc, s])
            expert(s)
            over(s).start()

        @pl.when(bundle(i, 5, i))
        def _():
            j = i - 5
            s = near(z, j)
            for side in range(2):
                await_bytes(upd.at[side, s], u_recv.at[side, s])
            for xh in range(2):
                total = r1[y, s, xh].astype(F32) + upd[0, s, xh].astype(F32) + upd[1, s, xh].astype(F32)
                fin[s, xh] = total.astype(BF16)
                own, copy = back(j, xh)

                @pl.when(own)
                def _(xh=xh):
                    ret[s, xh] = fin[s, xh]

                @pl.when(jnp.logical_not(own))
                def _(copy=copy):
                    copy.start()

        pl.when(i == 3)(join_row)
        pl.when(i == 6)(join_planes)
        pl.when(i == 7)(take_state)

        @pl.when(i >= 7)
        def _():
            for k in range(3):
                n = (i - 7) * 3 + k

                @pl.when(n < 16)
                def _(n=n):
                    pass_b_block(n, q_ref, k_ref, v_ref, g_ref, gain_ref, st, mixed)

        return carry

    lax.fori_loop(0, LAST, step, 0)

    def finish(j, carry):
        s = near(z, j)
        for xh in range(2):
            own, sent = exchange(j, xh)
            _, copy = back(j, xh)

            @pl.when(jnp.logical_not(own))
            def _(sent=sent, copy=copy, xh=xh):
                sent.wait_send()
                copy.wait_send()
                await_bytes(ret.at[s, xh], b_recv.at[s, xh])

        for copy in own_copies(s):
            copy.wait_send()
        await_bytes(low.at[s], f_send.at[s])
        for ysrc in range(NY):
            to_partner(ysrc, s).wait_send()
        over(s).wait_send()
        for sem in (l_send, u_send, t_send):
            await_bytes(low.at[s], sem.at[s])
        return carry

    lax.fori_loop(0, NZ, finish, 0)
    for zd in range(1, NZ):

        @pl.when(zd > z)
        def _(zd=zd):
            z_copy(zd).wait_send()

    for d in range(1, NX):
        x1(d).wait_send()
        x2(d).wait_send()

    weights = w_buf[...]
    w_hi = weights.astype(BF16)
    w_low = (weights - w_hi.astype(F32)).astype(BF16)

    def weigh(n, carry):
        at = pl.ds(pl.multiple_of(n * width, width), width)
        got_rows = ret[:, :, :, at].astype(F32).reshape(128, width).astype(BF16)
        got = lax.dot_general(w_hi, got_rows, TN, preferred_element_type=F32)
        got = got + lax.dot_general(w_low, got_rows, TN, preferred_element_type=F32)
        mine[:, at] = jnp.where(c == 0, got[0:32], got[32:64])
        cs[n] = jnp.where(c == 0, got[32:64], got[0:32])
        swap(n).start()
        return carry

    def swap(n):
        return remote(cs.at[n], cr.at[n], c_send.at[n], c_recv.at[n], c=1 - c)

    def join(n, carry):
        at = pl.ds(pl.multiple_of(n * width, width), width)
        swap(n).wait()
        mine[:, at] = mine[:, at] + cr[n]
        return carry

    lax.fori_loop(0, D // width, weigh, 0)
    lax.fori_loop(0, D // width, join, 0)
    total = mine[...]
    scale = lax.rsqrt(jnp.mean(total * total, axis=-1, keepdims=True) + 1e-6)
    routed[...] = (total * scale * post_ref[...]).astype(BF16)


def everything(picks, weights, pre, post, gain, rows, gate, up, down, q, k, v, g):
    dma = pltpu.SemaphoreType.DMA
    vmem = pl.BlockSpec(memory_space=pltpu.VMEM)
    hbm = pl.BlockSpec(memory_space=pl.ANY)
    scratch = [
        pltpu.VMEM((64, D), BF16),
        pltpu.VMEM(gate.shape, BF16),
        pltpu.VMEM(up.shape, BF16),
        pltpu.VMEM(down.shape, BF16),
        pltpu.VMEM(q.shape, BF16),
        pltpu.VMEM(k.shape, BF16),
        pltpu.VMEM(v.shape, BF16),
        pltpu.VMEM(g.shape, F32),
        pltpu.VMEM((16, 8, D), BF16),
        pltpu.VMEM((128, 64), F32),
        pltpu.VMEM((2, NY, NZ, 2, 8, D), BF16),
        pltpu.VMEM((128, D), BF16),
        pltpu.VMEM((2, NY, NZ, 2, 8, D), BF16),
        pltpu.VMEM((NY, NZ, 2, 8, D), BF16),
        pltpu.VMEM((NZ, 2, 8, D), BF16),
        pltpu.VMEM((2, NZ, 2, 8, D), BF16),
        pltpu.VMEM((NZ, 2, 8, D), BF16),
        pltpu.VMEM((NZ, 2, 8, D), BF16),
        pltpu.VMEM((32, D), F32),
        pltpu.VMEM((8, 32, D // 8), F32),
        pltpu.VMEM((8, 32, D // 8), F32),
        pltpu.VMEM((2, DV, DK), F32),
        pltpu.VMEM((1, 2 * DK), F32),
        pltpu.VMEM((4, 2, 80, DK), BF16),
        pltpu.VMEM((4, 2, 80, DK), BF16),
        pltpu.VMEM((2, 80, DK), BF16),
        pltpu.VMEM((NZ, 2, 80, DK), BF16),
        pltpu.VMEM((2, 64, DK), F32),
        pltpu.VMEM((4, 2, 64, DK), F32),
        pltpu.VMEM((4, 2, 64, DK), F32),
        dma((8,)), dma((NZ, 2)), dma((NZ, 2)), dma((2, NZ)), dma((NY, NZ)), dma((NZ,)), dma((NY, NZ)), dma((NY, NZ)),
        dma((3,)), dma((4,)), dma((NZ,)), dma((NZ,)), dma((3,)), dma((4,)),
        dma((NZ,)), dma((NZ,)), dma((NZ,)), dma((NZ,)), dma((NZ,)), dma((NZ,)), dma((2, NZ)),
        dma((NZ, 2)), dma((NZ, 2)), dma((8,)), dma((8,)),
    ]
    return pl.pallas_call(
        body,
        out_shape=(
            jax.ShapeDtypeStruct((1024, 2 * DV), BF16),
            jax.ShapeDtypeStruct((32, D), BF16),
        ),
        in_specs=[vmem] * 5 + [hbm] * 8,
        out_specs=[vmem, vmem],
        scratch_shapes=scratch,
        compiler_params=pltpu.CompilerParams(collective_id=0, has_side_effects=True, vmem_limit_bytes=VLIM),
        name="everything",
    )(picks, weights, pre, post, gain, rows, gate, up, down, q, k, v, g)


def on_device(
    queries,
    key_vectors,
    value_vectors,
    decay_logit,
    head_gain,
    routed_rows,
    pre_gain,
    expert_pick,
    route_weight,
    gate_weight,
    up_weight,
    down_weight,
    post_gain,
):
    return everything(
        expert_pick.T,
        route_weight.T,
        pre_gain.reshape(1, D),
        post_gain.reshape(1, D),
        head_gain.reshape(1, DV),
        routed_rows,
        gate_weight[0],
        up_weight[0],
        down_weight[0],
        queries,
        key_vectors,
        value_vectors,
        decay_logit,
    )


def solution(mesh):
    torus = Mesh(mesh.devices.reshape(NZ, NX, NY, 2), ("z", "x", "y", "c"))
    placed = (
        P(EP, TP),
        P(EP, TP),
        P(EP, TP),
        P(EP, TP),
        P(),
        P(EP, None),
        P(),
        P(EP, None),
        P(EP, None),
        P(EP, None, TP),
        P(EP, None, TP),
        P(EP, TP, None),
        P(),
    )
    return jax.shard_map(
        on_device,
        mesh=torus,
        in_specs=placed,
        out_specs=(P(EP, TP), P(EP + TP, None)),
        check_vma=False,
    )
```
